512 devices in a mesh: fs: 64 (over z, y), tp: 8 (over x, core).
Axes of the slice: x: 4, y: 4, z: 16, core: 2. Of those that a mesh axis runs over, the one named last changes fastest.
Arguments:
- tokens: bfloat16 [32768, 2048], P('fs', 'tp'), may hold values from -24 to 24
- u_weight: bfloat16 [2048, 1024], P('fs', 'tp'), may hold values from -0.125 to 0.125
- v_weight: bfloat16 [2048, 1024], P('fs', 'tp'), may hold values from -0.125 to 0.125
- sg_gain: float32 [1024], P('tp'), may hold values from 0.1 to 1.9
- spatial_weight: bfloat16 [8, 128, 128], P('tp'), may hold values from -0.5 to 0.5
- spatial_bias: float32 [8, 128], P('tp'), may hold values from 0.1 to 1.9
- out_weight: bfloat16 [1024, 2048], P('tp', 'fs'), may hold values from -0.1875 to 0.1875
- gain_one: float32 [2048], P('tp'), may hold values from 0.1 to 1.9
- gate_weight: bfloat16 [2048, 5632], P('fs', 'tp'), may hold values from -0.125 to 0.125
- up_weight: bfloat16 [2048, 5632], P('fs', 'tp'), may hold values from -0.125 to 0.125
- down_weight: bfloat16 [5632, 2048], P('tp', 'fs'), may hold values from -0.078125 to 0.078125
- gain_two: float32 [2048], P('tp'), may hold values from 0.1 to 1.9
Outputs:
- layer_out: bfloat16 [32768, 2048], P('fs', 'tp')
The draws below stay inside these ranges and needn't reach their ends.
All inputs are finite; a program needn't handle non-finite values.
Results may differ from the reference program's by a relative error of at most 0.014.
Values may be sent and summed in bfloat16 or wider, within the bound.
A program may use at most 64 MiB of HBM per device.

```python
import math
import jax
import jax.numpy as jnp
from jax import lax

D = 2048
FF = 5632
GROUPS = 8
GROUP_DIM = 128
BLOCK = 128
D_SG = 1024
TOKENS = 32768
N_TP = 8


def draw_tokens(key, part):
    first_key, second_key, third_key = jax.random.split(jax.random.fold_in(key, 11), 3)
    width = D // 16
    scales = jnp.exp(jax.random.uniform(second_key, (16,), jnp.float32, -math.log(4.0), math.log(4.0)))
    base = jax.random.normal(first_key, (TOKENS, D), jnp.float32)
    base = jnp.clip(base, -6.0, 6.0)
    return (base * jnp.repeat(scales, width)[None, :]).astype(jnp.bfloat16)


def steps_of(key, shape, pieces, least, high):
    factor_of, own = 1.0, jax.random.fold_in(key, 6)
    for position, blocks in pieces:
        draws = jnp.exp(jax.random.uniform(jax.random.fold_in(own, position), (blocks,), jnp.float32, least / len(pieces), high / len(pieces)))
        factor_of = factor_of * jnp.repeat(draws, shape[position] // blocks).reshape([-1 if axis == position else 1 for axis in range(len(shape))])
    return factor_of


def bell_draw(rng, extent, deviation, most, shards=(), kind=jnp.bfloat16):
    entries = deviation * jax.random.normal(rng, extent, jnp.float32)
    if shards:
        entries = entries * steps_of(rng, extent, shards, -0.22, 0.18)
    return jnp.clip(entries, -most, most).astype(kind)


def setup_inputs(seed: int = 0) -> dict:
    seeds = jax.random.split(jax.random.key(seed), 13)
    tokens = draw_tokens(jax.random.fold_in(seeds[12], 71), 0)
    u_weight = bell_draw(seeds[1], (D, D_SG), D ** -0.5, 0.125, ((0, 64), (1, 8)))
    v_weight = bell_draw(seeds[2], (D, D_SG), D ** -0.5, 0.125, ((0, 64), (1, 8)))
    sg_gain = jnp.clip(1.0 + 0.18 * jax.random.normal(seeds[3], (D_SG,), jnp.float32), 0.1, 1.9)
    spatial_weight = bell_draw(seeds[4], (GROUPS, BLOCK, BLOCK), BLOCK ** -0.5, 0.5, ((0, 8),))
    spatial_bias = jnp.clip(1.0 + 0.18 * jax.random.normal(seeds[5], (GROUPS, BLOCK), jnp.float32), 0.1, 1.9)
    out_weight = bell_draw(seeds[6], (D_SG, D), D_SG ** -0.5, 0.1875, ((0, 8), (1, 64)))
    gain_one = jnp.clip(1.0 + 0.18 * jax.random.normal(seeds[7], (D,), jnp.float32), 0.1, 1.9)
    gate_weight = bell_draw(seeds[8], (D, FF), D ** -0.5, 0.125, ((0, 64), (1, 8)))
    up_weight = bell_draw(seeds[9], (D, FF), D ** -0.5, 0.125, ((0, 64), (1, 8)))
    down_weight = bell_draw(seeds[10], (FF, D), FF ** -0.5, 0.078125, ((0, 8), (1, 64)))
    gain_two = jnp.clip(1.0 + 0.18 * jax.random.normal(seeds[11], (D,), jnp.float32), 0.1, 1.9)
    return {"tokens": tokens, "u_weight": u_weight, "v_weight": v_weight, "sg_gain": sg_gain, "spatial_weight": spatial_weight, "spatial_bias": spatial_bias, "out_weight": out_weight, "gain_one": gain_one, "gate_weight": gate_weight, "up_weight": up_weight, "down_weight": down_weight, "gain_two": gain_two}


EPS = 1e-05
ALPHA = 2.0 ** 0.25

def norm_rows(vals, gain):
    count = vals.shape[1]
    mean = lax.optimization_barrier(jnp.sum(vals, axis=1, keepdims=True)) / count
    square = lax.optimization_barrier(jnp.sum(vals * vals, axis=1, keepdims=True)) / count
    return (vals - mean) * lax.rsqrt(square - mean * mean + EPS) * gain.astype(jnp.float32)[None, :]

def split_sum(left, weight):
    width = weight.shape[0] // N_TP
    total = jnp.zeros((left.shape[0], weight.shape[1]), jnp.float32)
    for index in range(N_TP):
        part = jnp.dot(left[:, index * width:(index + 1) * width], weight[index * width:(index + 1) * width], preferred_element_type=jnp.float32).astype(jnp.bfloat16)
        part = lax.optimization_barrier(part)
        total = total + part.astype(jnp.float32)
    return total.astype(jnp.bfloat16)

def reference(tokens, u_weight, v_weight, sg_gain, spatial_weight, spatial_bias, out_weight, gain_one, gate_weight, up_weight, down_weight, gain_two):
    gated = jax.nn.gelu(jnp.dot(tokens, u_weight, preferred_element_type=jnp.float32))
    valued = jax.nn.gelu(jnp.dot(tokens, v_weight, preferred_element_type=jnp.float32))
    normed = norm_rows(valued, sg_gain).astype(jnp.bfloat16)
    blocks = TOKENS // BLOCK
    shaped = normed.reshape(blocks, BLOCK, GROUPS, GROUP_DIM).astype(jnp.float32)
    lower = jnp.tril(jnp.ones((BLOCK, BLOCK), jnp.float32))
    masked = spatial_weight.astype(jnp.float32) * lower[None]
    mixed = jnp.einsum('gij,njgd->nigd', masked, shaped)
    mixed = mixed + spatial_bias.astype(jnp.float32).T[None, :, :, None]
    gated_out = (gated * mixed.reshape(TOKENS, D_SG)).astype(jnp.bfloat16)
    mix = split_sum(gated_out, out_weight)
    first = norm_rows(ALPHA * tokens.astype(jnp.float32) + mix.astype(jnp.float32), gain_one).astype(jnp.bfloat16)
    gate = jnp.dot(first, gate_weight, preferred_element_type=jnp.float32)
    upper = jnp.dot(first, up_weight, preferred_element_type=jnp.float32)
    hidden = (jax.nn.silu(gate) * upper).astype(jnp.bfloat16)
    ffn = split_sum(hidden, down_weight)
    layer_out = norm_rows(ALPHA * first.astype(jnp.float32) + ffn.astype(jnp.float32), gain_two)
    return layer_out.astype(jnp.bfloat16)
```

```python
import jax
import jax.numpy as jnp
from jax import lax
from jax.experimental import pallas as pl
from jax.experimental.pallas import tpu as pltpu
from jax.sharding import PartitionSpec as P

EPS = 1e-05
ALPHA = 2.0**0.25
MESH = pl.DeviceIdType.MESH
ZN, YN, XN = 16, 4, 4
BF, F32 = jnp.bfloat16, jnp.float32


def wrap(value, size):
    return lax.rem(value + size, size)


def nt_dot(left, right, **kw):
    return lax.dot_general(left, right, (((1,), (1,)), ((), ())), preferred_element_type=F32, **kw)


class Place:
    def __init__(self):
        f, t = lax.axis_index("fs"), lax.axis_index("tp")
        self.f, self.t = f, t
        self.z, self.y = lax.div(f, YN), lax.rem(f, YN)
        self.x, self.c = lax.div(t, 2), lax.rem(t, 2)
        self.zp = (wrap(self.z + 1, ZN) * YN + self.y, t)
        self.zm = (wrap(self.z - 1, ZN) * YN + self.y, t)
        self.yp = (self.z * YN + wrap(self.y + 1, YN), t)
        self.ym = (self.z * YN + wrap(self.y - 1, YN), t)
        self.xp = (f, wrap(self.x + 1, XN) * 2 + self.c)
        self.xm = (f, wrap(self.x - 1, XN) * 2 + self.c)
        self.mate = (f, self.x * 2 + 1 - self.c)


def copy_to(src, dst, send, recv, dev):
    pltpu.make_async_remote_copy(src_ref=src, dst_ref=dst, send_sem=send, recv_sem=recv, device_id=dev, device_id_type=MESH).start()


def await_recv(dst, recv, dev):
    pltpu.make_async_remote_copy(src_ref=dst, dst_ref=dst, send_sem=recv, recv_sem=recv, device_id=dev, device_id_type=MESH).wait_recv()


def await_send(src, send, dev):
    pltpu.make_async_remote_copy(src_ref=src, dst_ref=src, send_sem=send, recv_sem=send, device_id=dev, device_id_type=MESH).wait_send()


class ZThenY:
    def __init__(self, w, f_sem, b_sem, yf_sem, yb_sem, last, sent, me):
        self.w, self.f_sem, self.b_sem, self.yf_sem, self.yb_sem = w, f_sem, b_sem, yf_sem, yb_sem
        self.last, self.sent, self.me = last, sent, me

    def block(self, zb, yb):
        row = (wrap(zb, ZN) * YN + wrap(yb, YN)) * 32
        return self.w.at[pl.ds(pl.multiple_of(row, 32), 32), :]

    def z(self, s):
        me = self.me
        fwd, bwd = self.block(me.z - s, me.y), self.block(me.z + s, me.y)
        if s > 0:
            await_recv(fwd, self.f_sem.at[s], me.zm)
        if s < 8:
            copy_to(fwd, fwd, self.sent, self.f_sem.at[s + 1], me.zp)
        if 0 < s < 8:
            await_recv(bwd, self.b_sem.at[s], me.zp)
        if s < 7:
            copy_to(bwd, bwd, self.sent, self.b_sem.at[s + 1], me.zm)

    def ys(self, s):
        me = self.me
        fwd, bwd = self.block(me.z - s, me.y), self.block(me.z + s, me.y)
        copy_to(fwd, fwd, self.sent, self.yf_sem.at[s], me.yp)
        copy_to(fwd, fwd, self.sent, self.last, me.ym)
        if 0 < s < 8:
            copy_to(bwd, bwd, self.sent, self.yb_sem.at[s], me.ym)
            copy_to(bwd, bwd, self.sent, self.last, me.yp)

    def yf(self, s):
        me = self.me
        fwd = self.block(me.z - s, me.y - 1)
        await_recv(fwd, self.yf_sem.at[s], me.ym)
        copy_to(fwd, fwd, self.sent, self.last, me.yp)
        if 0 < s < 8:
            bwd = self.block(me.z + s, me.y + 1)
            await_recv(bwd, self.yb_sem.at[s], me.yp)
            copy_to(bwd, bwd, self.sent, self.last, me.ym)

    def finish(self):
        await_recv(self.w.at[pl.ds(0, 1024), :], self.last, self.me.yp)

    def drain(self):
        await_send(self.w.at[pl.ds(0, 2016), :], self.sent, self.me.yp)


class YThenZ:
    def __init__(self, w, y_sem, f_sem, b_sem, sent, me):
        self.w, self.y_sem, self.f_sem, self.b_sem, self.sent, self.me = w, y_sem, f_sem, b_sem, sent, me

    def rows(self, yb, start, size):
        row = (self.me.z * YN + wrap(yb, YN)) * 32 + start
        return self.w.at[pl.ds(pl.multiple_of(row, 16), size), :]

    def block(self, zb):
        return self.w.at[pl.ds(pl.multiple_of(wrap(zb, ZN) * 128, 128), 128), :]

    def y0(self):
        me = self.me
        own = self.rows(me.y, 0, 32)
        copy_to(own, own, self.sent, self.y_sem.at[0], me.yp)
        copy_to(own, own, self.sent, self.y_sem.at[1], me.ym)

    def y1(self):
        me = self.me
        await_recv(self.rows(me.y - 1, 0, 32), self.y_sem.at[0], me.ym)
        half = self.rows(me.y - 1, 0, 16)
        copy_to(half, half, self.sent, self.y_sem.at[2], me.yp)
        await_recv(self.rows(me.y + 1, 0, 32), self.y_sem.at[1], me.yp)
        half = self.rows(me.y + 1, 16, 16)
        copy_to(half, half, self.sent, self.y_sem.at[3], me.ym)

    def y2(self):
        me = self.me
        await_recv(self.rows(me.y - 2, 0, 16), self.y_sem.at[2], me.ym)
        await_recv(self.rows(me.y + 2, 16, 16), self.y_sem.at[3], me.yp)

    def z(self, s):
        me = self.me
        fwd, bwd = self.block(me.z - s), self.block(me.z + s)
        if s > 0:
            await_recv(fwd, self.f_sem.at[s], me.zm)
        if s < 8:
            copy_to(fwd, fwd, self.sent, self.f_sem.at[s + 1], me.zp)
        if 0 < s < 8:
            await_recv(bwd, self.b_sem.at[s], me.zp)
        if s < 7:
            copy_to(bwd, bwd, self.sent, self.b_sem.at[s + 1], me.zm)

    def drain(self):
        await_send(self.w.at[pl.ds(0, 2016), :], self.sent, self.me.yp)


class Gather:
    def __init__(self, buf, sem, relayed, sent, me):
        self.buf, self.sem, self.relayed, self.sent, self.me = buf, sem, relayed, sent, me
        self.half = buf.shape[1] // 2

    def part(self, xb, h):
        b = wrap(xb, XN) * 2 + self.me.c
        return self.buf.at[b, pl.ds(h * self.half, self.half), :]

    def send(self, xb, h, sem, dev):
        part = self.part(xb, h)
        copy_to(part, part, self.sent, sem, dev)

    def take(self, xb, h, sem, dev):
        await_recv(self.part(xb, h), sem, dev)

    def start(self):
        me = self.me
        self.send(me.x, 0, self.sem.at[0], me.xp)
        self.send(me.x, 1, self.sem.at[3], me.xm)
        self.send(me.x, 1, self.sem.at[1], me.xp)
        self.send(me.x, 0, self.sem.at[2], me.xm)
        own = self.buf.at[me.t]
        copy_to(own, own, self.sent, self.relayed, me.mate)

    def forward(self):
        me = self.me
        self.take(me.x - 1, 0, self.sem.at[0], me.xm)
        self.send(me.x - 1, 0, self.sem.at[4], me.xp)
        self.send(me.x - 1, 0, self.relayed, me.mate)
        self.take(me.x + 1, 1, self.sem.at[3], me.xp)
        self.send(me.x + 1, 1, self.sem.at[5], me.xm)
        self.send(me.x + 1, 1, self.relayed, me.mate)

    def middle(self):
        me = self.me
        self.take(me.x - 1, 1, self.sem.at[1], me.xm)
        self.send(me.x - 1, 1, self.relayed, me.mate)
        self.take(me.x + 1, 0, self.sem.at[2], me.xp)
        self.send(me.x + 1, 0, self.relayed, me.mate)

    def end(self):
        me = self.me
        self.take(me.x - 2, 0, self.sem.at[4], me.xm)
        self.send(me.x - 2, 0, self.relayed, me.mate)
        self.take(me.x + 2, 1, self.sem.at[5], me.xp)
        self.send(me.x + 2, 1, self.relayed, me.mate)

    def finish(self):
        await_recv(self.buf.at[pl.ds(0, 4)], self.relayed, self.me.mate)

    def drain(self):
        await_send(self.buf.at[pl.ds(0, 7)], self.sent, self.me.mate)


class Scatter:
    def __init__(self, part, other, total, via, got, sem, sent, me):
        self.part, self.other, self.total, self.via, self.got = part, other, total, via, got
        self.sem, self.sent, self.me = sem, sent, me
        self.half = part.shape[1] // 2

    def swap(self, d):
        me = self.me
        xb = wrap(me.x + d, XN)
        copy_to(self.part.at[xb * 2 + 1 - me.c], self.other.at[d], self.sent, self.sem.at[d], me.mate)

    def add(self, d):
        me = self.me
        xb = wrap(me.x + d, XN)
        await_recv(self.other.at[d], self.sem.at[d], me.mate)
        return self.part[xb * 2 + me.c].astype(F32) + self.other[d].astype(F32)

    def rows(self, h):
        return pl.ds(h * self.half, self.half)

    def far(self):
        me = self.me
        self.total[2] = self.add(2).astype(BF)
        copy_to(self.total.at[2, self.rows(0), :], self.via.at[0], self.sent, self.sem.at[4], me.xp)
        copy_to(self.total.at[2, self.rows(1), :], self.via.at[1], self.sent, self.sem.at[5], me.xm)

    def near(self):
        me = self.me
        self.total[1] = self.add(1).astype(BF)
        copy_to(self.total.at[1, self.rows(1), :], self.got.at[0, self.rows(1), :], self.sent, self.sem.at[6], me.xp)
        self.total[3] = self.add(3).astype(BF)
        copy_to(self.total.at[3, self.rows(0), :], self.got.at[1, self.rows(0), :], self.sent, self.sem.at[7], me.xm)

    def hop(self):
        me = self.me
        await_recv(self.via.at[0], self.sem.at[4], me.xm)
        self.total[1, self.rows(0), :] = (self.total[1, self.rows(0), :].astype(F32) + self.via[0].astype(F32)).astype(BF)
        copy_to(self.total.at[1, self.rows(0), :], self.got.at[0, self.rows(0), :], self.sent, self.sem.at[8], me.xp)
        await_recv(self.via.at[1], self.sem.at[5], me.xp)
        self.total[3, self.rows(1), :] = (self.total[3, self.rows(1), :].astype(F32) + self.via[1].astype(F32)).astype(BF)
        copy_to(self.total.at[3, self.rows(1), :], self.got.at[1, self.rows(1), :], self.sent, self.sem.at[9], me.xm)

    def result(self):
        me = self.me
        own = self.add(0)
        await_recv(self.got.at[0, self.rows(1), :], self.sem.at[6], me.xm)
        await_recv(self.got.at[1, self.rows(0), :], self.sem.at[7], me.xp)
        await_recv(self.got.at[0, self.rows(0), :], self.sem.at[8], me.xm)
        await_recv(self.got.at[1, self.rows(1), :], self.sem.at[9], me.xp)
        return (own + self.got[0].astype(F32) + self.got[1].astype(F32)).astype(BF).astype(F32)

    def drain(self):
        await_send(self.part.at[pl.ds(0, 7)], self.sent, self.me.mate)


def everyone(me, buf, recv, sent):
    own = buf.at[me.t]
    for d in range(1, 8):
        copy_to(own, own, sent, recv.at[d], (me.f, wrap(me.t + d, 8)))


def from_everyone(me, buf, recv):
    for d in range(1, 8):
        t = wrap(me.t - d, 8)
        await_recv(buf.at[t], recv.at[d], (me.f, t))


def drain_everyone(me, buf, sent):
    await_send(buf.at[pl.ds(0, 7)], sent, (me.f, wrap(me.t + 1, 8)))


def row_sums(vals):
    ones = jnp.ones((8, vals.shape[1]), F32)
    return nt_dot(ones, vals, precision=lax.Precision.HIGHEST)[0:1]


def spread(line, rows=128):
    return jnp.broadcast_to(line, (rows, line.shape[1])).T


def kernel(
    tok, u, v, sgg, sw, sb, ow, g1, gw, uw, dw, g2, out,
    wuv, wo, wgu, wd, tall, first, gains, stat1, stat2,
    part1, other1, total1, via1, got1, part2, other2, total2, via2, got2,
    gated, valued, hidden,
    uv_f, uv_b, uv_yf, uv_yb, gu_f, gu_b, gu_yf, gu_yb, wo_y, wo_f, wo_b, wd_y, wd_f, wd_b,
    ag1_s, ag2_s, rs1_s, rs2_s, gain_s, st1_s, st2_s, one,
):
    me = Place()
    barrier = pltpu.get_barrier_semaphore()
    for dev in (me.zp, me.zm, me.yp, me.ym):
        pl.semaphore_signal(barrier, inc=1, device_id=dev, device_id_type=MESH)
    for d in range(1, 8):
        pl.semaphore_signal(barrier, inc=1, device_id=(me.f, wrap(me.t + d, 8)), device_id_type=MESH)

    rows = pl.ds(pl.multiple_of(me.f * 32, 32), 32)
    eye = (lax.broadcasted_iota(jnp.int32, (32, 32), 0) == lax.broadcasted_iota(jnp.int32, (32, 32), 1)).astype(BF)
    lane = lax.broadcasted_iota(jnp.int32, (64, 128), 1)
    line = lax.broadcasted_iota(jnp.int32, (64, 128), 0)
    low, high = (lane == line).astype(BF), (lane == line + 64).astype(BF)
    wuv[rows, 0:128] = u[...]
    wuv[rows, 128:256] = v[...]
    wo[rows, :] = nt_dot(eye, ow[...]).astype(BF)
    for n in range(5):
        wgu[rows, n * 256 : n * 256 + 128] = gw[:, n * 128 : (n + 1) * 128]
        wgu[rows, n * 256 + 128 : n * 256 + 256] = uw[:, n * 128 : (n + 1) * 128]
    tail = jnp.dot(gw[:, 640:704], low, preferred_element_type=F32) + jnp.dot(uw[:, 640:704], high, preferred_element_type=F32)
    wgu[rows, 1280:1408] = tail.astype(BF)
    wd[rows, 640:768] = jnp.zeros((32, 128), BF)
    wd[rows, 0:704] = nt_dot(eye, dw[...]).astype(BF)
    tall[me.t] = tok[...]
    gains[me.t] = g1[...]
    pl.semaphore_wait(barrier, 11)

    uv = ZThenY(wuv, uv_f, uv_b, uv_yf, uv_yb, one.at[0], one.at[1], me)
    gu = ZThenY(wgu, gu_f, gu_b, gu_yf, gu_yb, one.at[2], one.at[3], me)
    ot = YThenZ(wo, wo_y, wo_f, wo_b, one.at[4], me)
    dn = YThenZ(wd, wd_y, wd_f, wd_b, one.at[5], me)
    ag1 = Gather(tall, ag1_s, one.at[6], one.at[7], me)
    ag2 = Gather(first, ag2_s, one.at[8], one.at[9], me)
    rs1 = Scatter(part1, other1, total1, via1, got1, rs1_s, one.at[10], me)
    rs2 = Scatter(part2, other2, total2, via2, got2, rs2_s, one.at[11], me)

    uv.z(0)
    uv.ys(0)
    ag1.start()
    ot.y0()
    everyone(me, gains, gain_s, one.at[12])
    gu.z(0)
    gu.ys(0)
    dn.y0()

    uv.z(1)
    uv.ys(1)
    uv.yf(0)
    ot.y1()
    dn.y1()

    uv.z(2)
    uv.ys(2)
    uv.yf(1)
    ot.y2()
    ot.z(0)
    gu.yf(0)
    gu.z(1)
    ag1.forward()

    uv.z(3)
    uv.ys(3)
    uv.yf(2)
    ot.z(1)
    gu.ys(1)
    dn.y2()

    uv.z(4)
    uv.ys(4)
    uv.yf(3)
    ot.z(2)
    gu.z(2)
    ag1.middle()

    uv.z(5)
    uv.ys(5)
    uv.yf(4)
    ot.z(3)
    gu.yf(1)

    uv.z(6)
    uv.ys(6)
    uv.yf(5)
    ot.z(4)
    ag1.end()

    uv.z(7)
    uv.ys(7)
    uv.yf(6)
    ot.z(5)
    gu.z(3)

    uv.z(8)
    uv.ys(8)
    uv.yf(7)
    ot.z(6)
    uv.yf(8)
    gu.ys(2)
    dn.z(0)
    ot.z(7)
    ag1.finish()
    uv.finish()

    pre = jnp.dot(
        jnp.concatenate([tall[k] for k in range(8)], axis=1), wuv[...], preferred_element_type=F32
    )
    gated[...] = jax.nn.gelu(pre[:, 0:128])
    val = jax.nn.gelu(pre[:, 128:256])
    valued[...] = val
    stat1[me.t] = jnp.concatenate([row_sums(val), row_sums(val * val)], axis=0)
    everyone(me, stat1, st1_s, one.at[13])
    gu.yf(2)
    gu.ys(3)
    ot.z(8)
    from_everyone(me, stat1, st1_s)
    sums = jnp.sum(stat1[...], axis=0)
    mean = sums[0:1] / 1024.0
    rstd = lax.rsqrt(sums[1:2] / 1024.0 - mean * mean + EPS)
    normed = ((valued[...] - spread(mean)) * spread(rstd) * sgg[...]).astype(BF)
    keep = lax.broadcasted_iota(jnp.int32, (128, 128), 0) >= lax.broadcasted_iota(jnp.int32, (128, 128), 1)
    mask = jnp.where(keep, sw[0].astype(F32), 0.0).astype(BF)
    bias = spread(sb[...])
    wide = jnp.concatenate([normed[k * 128 : (k + 1) * 128] for k in range(4)], axis=1)
    mixed = jnp.dot(mask, wide, preferred_element_type=F32)
    go = jnp.concatenate(
        [gated[k * 128 : (k + 1) * 128, :] * (mixed[:, k * 128 : (k + 1) * 128] + bias) for k in range(4)], axis=0
    ).astype(BF)
    for n in range(8):
        cols = nt_dot(go, wo[n * 256 : (n + 1) * 256, :]).astype(BF)
        part1[:, :, n * 256 : (n + 1) * 256] = cols.reshape(8, 64, 256)
    for d in (2, 1, 3, 0):
        rs1.swap(d)
    gu.z(4)
    gu.ys(4)
    gu.yf(3)
    rs1.far()
    rs1.near()
    dn.z(1)
    gu.z(5)
    gu.ys(5)
    gu.yf(4)
    rs1.hop()
    dn.z(2)
    gu.z(6)
    mix = rs1.result()

    mine = pl.ds(pl.multiple_of(me.t * 64, 64), 64)
    held = jnp.concatenate([tall[k, mine, :] for k in range(8)], axis=1).astype(F32)
    resid = ALPHA * held + mix
    from_everyone(me, gains, gain_s)
    gain = jnp.concatenate([gains[k] for k in range(8)], axis=1)
    mean = jnp.sum(resid, axis=1, keepdims=True) / 2048.0
    square = jnp.sum(resid * resid, axis=1, keepdims=True) / 2048.0
    first[me.t] = ((resid - mean) * lax.rsqrt(square - mean * mean + EPS) * gain).astype(BF)
    ag2.start()
    gu.ys(6)
    gu.yf(5)
    dn.z(3)
    ag2.forward()
    gu.z(7)
    gu.ys(7)
    gu.yf(6)
    ag2.middle()
    dn.z(4)
    gu.z(8)
    gu.ys(8)
    ag2.end()
    gu.yf(7)
    dn.z(5)
    gu.yf(8)
    ag2.finish()
    gu.finish()

    for n in range(5):
        acc = jnp.dot(first[...].reshape(512, 2048), wgu[:, n * 256 : (n + 1) * 256], preferred_element_type=F32)
        hidden[:, n * 128 : (n + 1) * 128] = (jax.nn.silu(acc[:, 0:128]) * acc[:, 128:256]).astype(BF)
        if n == 1:
            dn.z(6)
        if n == 4:
            dn.z(7)
    acc = jnp.dot(first[...].reshape(512, 2048), wgu[:, 1280:1408], preferred_element_type=F32)
    prod = jax.nn.silu(acc) * pltpu.roll(acc, 64, axis=1)
    real = lax.broadcasted_iota(jnp.int32, (512, 128), 1) < 64
    hidden[:, 640:768] = jnp.where(real, prod, 0.0).astype(BF)
    dn.z(8)
    for n in range(8):
        part2[n] = nt_dot(hidden[...], wd[n * 256 : (n + 1) * 256, :]).astype(BF)
    for d in (2, 1, 3, 0):
        rs2.swap(d)
    rs2.far()
    rs2.near()
    rs2.hop()
    ffn = rs2.result()

    here = pl.ds(pl.multiple_of(me.t * 256, 256), 256)
    second = ALPHA * first[:, :, here].reshape(512, 256).astype(F32) + ffn
    stat2[me.t] = jnp.concatenate([row_sums(second), row_sums(second * second)], axis=0)
    everyone(me, stat2, st2_s, one.at[14])
    from_everyone(me, stat2, st2_s)
    sums = jnp.sum(stat2[...], axis=0)
    mean = sums[0:1] / 2048.0
    rstd = lax.rsqrt(sums[1:2] / 2048.0 - mean * mean + EPS)
    mean, rstd = spread(mean), spread(rstd)
    for k in range(2):
        span = slice(k * 128, (k + 1) * 128)
        out[:, span] = ((second[:, span] - mean) * rstd * g2[:, span]).astype(BF)

    uv.drain()
    gu.drain()
    ot.drain()
    dn.drain()
    ag1.drain()
    ag2.drain()
    rs1.drain()
    rs2.drain()
    drain_everyone(me, gains, one.at[12])
    drain_everyone(me, stat1, one.at[13])
    drain_everyone(me, stat2, one.at[14])


def on_device(tokens, u, v, sgg, sw, sb, ow, g1, gw, uw, dw, g2):
    vmem = pltpu.VMEM
    dma = pltpu.SemaphoreType.DMA
    scatter1 = [vmem((8, 64, 2048), BF), vmem((4, 64, 2048), BF), vmem((4, 64, 2048), BF), vmem((2, 32, 2048), BF), vmem((2, 64, 2048), BF)]
    scatter2 = [vmem((8, 512, 256), BF), vmem((4, 512, 256), BF), vmem((4, 512, 256), BF), vmem((2, 256, 256), BF), vmem((2, 512, 256), BF)]
    scratch = [
        vmem((2048, 256), BF), vmem((2048, 128), BF), vmem((2048, 1408), BF), vmem((2048, 768), BF),
        vmem((8, 512, 256), BF), vmem((8, 64, 2048), BF), vmem((8, 1, 256), F32), vmem((8, 2, 512), F32), vmem((8, 2, 512), F32),
        *scatter1, *scatter2,
        vmem((512, 128), F32), vmem((512, 128), F32), vmem((512, 768), BF),
        *[dma((9,)) for _ in range(8)],
        *[dma((4,)), dma((9,)), dma((9,))] * 2,
        dma((6,)), dma((6,)), dma((10,)), dma((10,)), dma((8,)), dma((8,)), dma((8,)), dma((16,)),
    ]
    return pl.pallas_call(
        kernel,
        out_shape=jax.ShapeDtypeStruct((512, 256), BF),
        in_specs=[pl.BlockSpec(memory_space=pltpu.VMEM)] * 12,
        out_specs=pl.BlockSpec(memory_space=pltpu.VMEM),
        scratch_shapes=scratch,
        compiler_params=pltpu.CompilerParams(collective_id=0, has_side_effects=True, vmem_limit_bytes=60 * 1024 * 1024),
    )(tokens, u, v, sgg.reshape(1, -1), sw, sb, ow, g1.reshape(1, -1), gw, uw, dw, g2.reshape(1, -1))


def solution(mesh):
    fs_tp, tp = P("fs", "tp"), P("tp")
    return jax.shard_map(
        on_device,
        mesh=mesh,
        in_specs=(
            fs_tp, fs_tp, fs_tp, tp, P("tp", None, None), P("tp", None), P("tp", "fs"), tp, fs_tp, fs_tp, P("tp", "fs"), tp,
        ),
        out_specs=fs_tp,
        check_vma=False,
    )
```

```python
import jax
import jax.numpy as jnp
from jax import lax
from jax.experimental import pallas as pl
from jax.experimental.pallas import tpu as pltpu
from jax.sharding import PartitionSpec as P

EPS = 1e-05
ALPHA = 2.0**0.25
MESH = pl.DeviceIdType.MESH
ZN, YN, XN = 16, 4, 4
BF, F32 = jnp.bfloat16, jnp.float32


def wrap(value, size):
    return lax.rem(value + size, size)


def nt_dot(left, right, **kw):
    return lax.dot_general(left, right, (((1,), (1,)), ((), ())), preferred_element_type=F32, **kw)


class Place:
    def __init__(self):
        f, t = lax.axis_index("fs"), lax.axis_index("tp")
        self.f, self.t = f, t
        self.z, self.y = lax.div(f, YN), lax.rem(f, YN)
        self.x, self.c = lax.div(t, 2), lax.rem(t, 2)
        self.zp = (wrap(self.z + 1, ZN) * YN + self.y, t)
        self.zm = (wrap(self.z - 1, ZN) * YN + self.y, t)
        self.yp = (self.z * YN + wrap(self.y + 1, YN), t)
        self.ym = (self.z * YN + wrap(self.y - 1, YN), t)
        self.xp = (f, wrap(self.x + 1, XN) * 2 + self.c)
        self.xm = (f, wrap(self.x - 1, XN) * 2 + self.c)
        self.mate = (f, self.x * 2 + 1 - self.c)

    def along_z(self, n):
        return (wrap(self.z + n, ZN) * YN + self.y, self.t)


def copy_to(src, dst, send, recv, dev):
    pltpu.make_async_remote_copy(src_ref=src, dst_ref=dst, send_sem=send, recv_sem=recv, device_id=dev, device_id_type=MESH).start()


def await_recv(dst, recv, dev):
    pltpu.make_async_remote_copy(src_ref=dst, dst_ref=dst, send_sem=recv, recv_sem=recv, device_id=dev, device_id_type=MESH).wait_recv()


def await_send(src, send, dev):
    pltpu.make_async_remote_copy(src_ref=src, dst_ref=src, send_sem=send, recv_sem=send, device_id=dev, device_id_type=MESH).wait_send()


class ZThenY:
    def __init__(self, w, f_sem, b_sem, yf_sem, yb_sem, last, sent, me, hops=1, split=9):
        self.w, self.f_sem, self.b_sem, self.yf_sem, self.yb_sem = w, f_sem, b_sem, yf_sem, yb_sem
        self.last, self.sent, self.me, self.hops, self.split = last, sent, me, hops, split

    def block(self, zb, yb):
        row = (wrap(zb, ZN) * YN + wrap(yb, YN)) * 32
        return self.w.at[pl.ds(pl.multiple_of(row, 32), 32), :]

    def final(self, s):
        return self.last.at[0 if s < self.split else 1]

    def z(self, s):
        me = self.me
        fwd, bwd = self.block(me.z - s, me.y), self.block(me.z + s, me.y)
        steps = range(1, self.hops + 1) if s == 0 else (self.hops,)
        if s > 0:
            await_recv(fwd, self.f_sem.at[s], me.zm)
        for n in steps:
            if s + n <= 8:
                copy_to(fwd, fwd, self.sent, self.f_sem.at[s + n], me.along_z(n))
        if 0 < s < 8:
            await_recv(bwd, self.b_sem.at[s], me.zp)
        for n in steps:
            if s + n <= 7:
                copy_to(bwd, bwd, self.sent, self.b_sem.at[s + n], me.along_z(-n))

    def up(self, s, block):
        me = self.me
        copy_to(block, block, self.sent, self.yf_sem.at[s], me.yp)
        copy_to(block, block, self.sent, self.final(s), me.ym)

    def down(self, s, block):
        me = self.me
        copy_to(block, block, self.sent, self.yb_sem.at[s], me.ym)
        copy_to(block, block, self.sent, self.final(s), me.yp)

    def ys(self, s):
        me = self.me
        if s < 8:
            self.up(s, self.block(me.z - s, me.y))
        if s > 0:
            self.down(s, self.block(me.z + s, me.y))

    def yf(self, s):
        me = self.me
        if s < 8:
            block = self.block(me.z - s, me.y - 1)
            await_recv(block, self.yf_sem.at[s], me.ym)
            copy_to(block, block, self.sent, self.final(s), me.yp)
        if s > 0:
            block = self.block(me.z + s, me.y + 1)
            await_recv(block, self.yb_sem.at[s], me.yp)
            copy_to(block, block, self.sent, self.final(s), me.ym)

    def finish(self):
        zs = 2 * self.split - 1 if self.split < 9 else ZN
        await_recv(self.w.at[pl.ds(0, zs * 64), :], self.last.at[0], self.me.yp)

    def finish_rest(self):
        zs = ZN - (2 * self.split - 1)
        await_recv(self.w.at[pl.ds(0, zs * 64), :], self.last.at[1], self.me.yp)

    def drain(self):
        await_send(self.w.at[pl.ds(0, 2016), :], self.sent, self.me.yp)


class YThenZ:
    def __init__(self, w, y_sem, f_sem, b_sem, sent, me):
        self.w, self.y_sem, self.f_sem, self.b_sem, self.sent, self.me = w, y_sem, f_sem, b_sem, sent, me

    def rows(self, yb, start, size):
        row = (self.me.z * YN + wrap(yb, YN)) * 32 + start
        return self.w.at[pl.ds(pl.multiple_of(row, 16), size), :]

    def block(self, zb, h):
        return self.w.at[pl.ds(pl.multiple_of(wrap(zb, ZN) * 128 + h * 64, 64), 64), :]

    def y0(self):
        me = self.me
        own = self.rows(me.y, 0, 32)
        copy_to(own, own, self.sent, self.y_sem.at[0], me.yp)
        copy_to(own, own, self.sent, self.y_sem.at[1], me.ym)

    def y1(self):
        me = self.me
        await_recv(self.rows(me.y - 1, 0, 32), self.y_sem.at[0], me.ym)
        half = self.rows(me.y - 1, 0, 16)
        copy_to(half, half, self.sent, self.y_sem.at[2], me.yp)
        await_recv(self.rows(me.y + 1, 0, 32), self.y_sem.at[1], me.yp)
        half = self.rows(me.y + 1, 16, 16)
        copy_to(half, half, self.sent, self.y_sem.at[3], me.ym)

    def y2(self):
        me = self.me
        await_recv(self.rows(me.y - 2, 0, 16), self.y_sem.at[2], me.ym)
        await_recv(self.rows(me.y + 2, 16, 16), self.y_sem.at[3], me.yp)

    def z(self, s, halves=(0, 1)):
        me = self.me
        for h in halves:
            fwd, bwd = self.block(me.z - s, h), self.block(me.z + s, h)
            if 0 < s < 8 or (s == 8 and h == 0):
                await_recv(fwd, self.f_sem.at[h * 9 + s], me.zm)
            if s < 7 or (s == 7 and h == 0):
                copy_to(fwd, fwd, self.sent, self.f_sem.at[h * 9 + s + 1], me.zp)
            if 0 < s < 8 or (s == 8 and h == 1):
                await_recv(bwd, self.b_sem.at[h * 9 + s], me.zp)
            if s < 7 or (s == 7 and h == 1):
                copy_to(bwd, bwd, self.sent, self.b_sem.at[h * 9 + s + 1], me.zm)

    def drain(self):
        await_send(self.w.at[pl.ds(0, 2016), :], self.sent, self.me.yp)


class Gather:
    def __init__(self, buf, sem, relayed, sent, me):
        self.buf, self.sem, self.relayed, self.sent, self.me = buf, sem, relayed, sent, me
        self.half = buf.shape[1] // 2

    def part(self, xb, h):
        b = wrap(xb, XN) * 2 + self.me.c
        return self.buf.at[b, pl.ds(h * self.half, self.half), :]

    def send(self, xb, h, sem, dev):
        part = self.part(xb, h)
        copy_to(part, part, self.sent, sem, dev)

    def take(self, xb, h, sem, dev):
        await_recv(self.part(xb, h), sem, dev)

    def start(self):
        me = self.me
        self.send(me.x, 0, self.sem.at[0], me.xp)
        self.send(me.x, 1, self.sem.at[3], me.xm)
        self.send(me.x, 1, self.sem.at[1], me.xp)
        self.send(me.x, 0, self.sem.at[2], me.xm)
        own = self.buf.at[me.t]
        copy_to(own, own, self.sent, self.relayed, me.mate)

    def forward(self):
        me = self.me
        self.take(me.x - 1, 0, self.sem.at[0], me.xm)
        self.send(me.x - 1, 0, self.sem.at[4], me.xp)
        self.send(me.x - 1, 0, self.relayed, me.mate)
        self.take(me.x + 1, 1, self.sem.at[3], me.xp)
        self.send(me.x + 1, 1, self.sem.at[5], me.xm)
        self.send(me.x + 1, 1, self.relayed, me.mate)

    def middle(self):
        me = self.me
        self.take(me.x - 1, 1, self.sem.at[1], me.xm)
        self.send(me.x - 1, 1, self.relayed, me.mate)
        self.take(me.x + 1, 0, self.sem.at[2], me.xp)
        self.send(me.x + 1, 0, self.relayed, me.mate)

    def end(self):
        me = self.me
        self.take(me.x - 2, 0, self.sem.at[4], me.xm)
        self.send(me.x - 2, 0, self.relayed, me.mate)
        self.take(me.x + 2, 1, self.sem.at[5], me.xp)
        self.send(me.x + 2, 1, self.relayed, me.mate)

    def finish(self):
        await_recv(self.buf.at[pl.ds(0, 4)], self.relayed, self.me.mate)

    def drain(self):
        await_send(self.buf.at[pl.ds(0, 7)], self.sent, self.me.mate)


class Scatter:
    def __init__(self, part, other, total, via, got, sem, sent, me):
        self.part, self.other, self.total, self.via, self.got = part, other, total, via, got
        self.sem, self.sent, self.me = sem, sent, me
        self.half = part.shape[1] // 2

    def swap(self, d):
        me = self.me
        xb = wrap(me.x + d, XN)
        copy_to(self.part.at[xb * 2 + 1 - me.c], self.other.at[d], self.sent, self.sem.at[d], me.mate)

    def add(self, d):
        me = self.me
        xb = wrap(me.x + d, XN)
        await_recv(self.other.at[d], self.sem.at[d], me.mate)
        return self.part[xb * 2 + me.c].astype(F32) + self.other[d].astype(F32)

    def rows(self, h):
        return pl.ds(h * self.half, self.half)

    def far(self):
        me = self.me
        self.total[2] = self.add(2).astype(BF)
        copy_to(self.total.at[2, self.rows(0), :], self.via.at[0], self.sent, self.sem.at[4], me.xp)
        copy_to(self.total.at[2, self.rows(1), :], self.via.at[1], self.sent, self.sem.at[5], me.xm)

    def near(self):
        me = self.me
        self.total[1] = self.add(1).astype(BF)
        copy_to(self.total.at[1, self.rows(1), :], self.got.at[0, self.rows(1), :], self.sent, self.sem.at[6], me.xp)
        self.total[3] = self.add(3).astype(BF)
        copy_to(self.total.at[3, self.rows(0), :], self.got.at[1, self.rows(0), :], self.sent, self.sem.at[7], me.xm)

    def hop(self):
        me = self.me
        await_recv(self.via.at[0], self.sem.at[4], me.xm)
        self.total[1, self.rows(0), :] = (self.total[1, self.rows(0), :].astype(F32) + self.via[0].astype(F32)).astype(BF)
        copy_to(self.total.at[1, self.rows(0), :], self.got.at[0, self.rows(0), :], self.sent, self.sem.at[8], me.xp)
        await_recv(self.via.at[1], self.sem.at[5], me.xp)
        self.total[3, self.rows(1), :] = (self.total[3, self.rows(1), :].astype(F32) + self.via[1].astype(F32)).astype(BF)
        copy_to(self.total.at[3, self.rows(1), :], self.got.at[1, self.rows(1), :], self.sent, self.sem.at[9], me.xm)

    def result(self):
        me = self.me
        own = self.add(0)
        await_recv(self.got.at[0, self.rows(1), :], self.sem.at[6], me.xm)
        await_recv(self.got.at[1, self.rows(0), :], self.sem.at[7], me.xp)
        await_recv(self.got.at[0, self.rows(0), :], self.sem.at[8], me.xm)
        await_recv(self.got.at[1, self.rows(1), :], self.sem.at[9], me.xp)
        return (own + self.got[0].astype(F32) + self.got[1].astype(F32)).astype(BF).astype(F32)

    def drain(self):
        await_send(self.part.at[pl.ds(0, 7)], self.sent, self.me.mate)


def everyone(me, buf, recv, sent):
    own = buf.at[me.t]
    for d in range(1, 8):
        copy_to(own, own, sent, recv.at[d], (me.f, wrap(me.t + d, 8)))


def from_everyone(me, buf, recv):
    for d in range(1, 8):
        t = wrap(me.t - d, 8)
        await_recv(buf.at[t], recv.at[d], (me.f, t))


def drain_everyone(me, buf, sent):
    await_send(buf.at[pl.ds(0, 7)], sent, (me.f, wrap(me.t + 1, 8)))


def row_sums(vals):
    ones = jnp.ones((8, vals.shape[1]), F32)
    return nt_dot(ones, vals, precision=lax.Precision.HIGHEST)[0:1]


def spread(line, rows=128):
    return jnp.broadcast_to(line, (rows, line.shape[1])).T


def kernel(
    tok, u, v, sgg_in, sw_in, sb_in, ow, g1, gw_in, uw_in, dw_in, g2_in, out,
    wuv, wo, wgu, wd, tall, first, gains, stat1, stat2,
    part1, other1, total1, via1, got1, part2, other2, total2, via2, got2,
    gated, valued, mixed_in, sums_in, hidden, sgg, sw, sb, gw, uw, dw, g2,
    uv_f, uv_b, uv_yf, uv_yb, wo_f, wo_b, wo_yf, wo_yb, gu_f, gu_b, gu_yf, gu_yb, wd_y, wd_f, wd_b,
    ag1_s, ag2_s, rs1_s, rs2_s, gain_s, st1_s, st2_s, one, in_s,
):
    me = Place()
    barrier = pltpu.get_barrier_semaphore()
    for dev in (me.zp, me.zm, me.along_z(2), me.along_z(-2), me.yp, me.ym):
        pl.semaphore_signal(barrier, inc=1, device_id=dev, device_id_type=MESH)
    for d in range(1, 8):
        pl.semaphore_signal(barrier, inc=1, device_id=(me.f, wrap(me.t + d, 8)), device_id_type=MESH)

    rows = pl.ds(pl.multiple_of(me.f * 32, 32), 32)
    loads = [
        pltpu.make_async_copy(src, dst, in_s.at[k])
        for k, (src, dst) in enumerate(
            (
                (u, wuv.at[rows, pl.ds(0, 128)]), (v, wuv.at[rows, pl.ds(128, 128)]), (ow, wo.at[rows, :]),
                (tok, tall.at[me.t]), (g1, gains.at[me.t]), (gw_in, gw), (uw_in, uw), (dw_in, dw),
                (sgg_in, sgg), (sw_in, sw), (sb_in, sb), (g2_in, g2),
            )
        )
    ]
    for load in loads:
        load.start()
    lane = lax.broadcasted_iota(jnp.int32, (64, 128), 1)
    line = lax.broadcasted_iota(jnp.int32, (64, 128), 0)
    low, high = (lane == line).astype(BF), (lane == line + 64).astype(BF)
    for load in loads:
        load.wait()
    for n in range(5):
        wgu[rows, n * 256 : n * 256 + 128] = gw[:, n * 128 : (n + 1) * 128]
        wgu[rows, n * 256 + 128 : n * 256 + 256] = uw[:, n * 128 : (n + 1) * 128]
    tail = jnp.dot(gw[:, 640:704], low, preferred_element_type=F32) + jnp.dot(uw[:, 640:704], high, preferred_element_type=F32)
    wd[rows, 768:896] = tail.astype(BF)
    wd[rows, 640:768] = jnp.zeros((32, 128), BF)
    wd[rows, 0:704] = dw[...]
    pl.semaphore_wait(barrier, 13)

    uv = ZThenY(wuv, uv_f, uv_b, uv_yf, uv_yb, one.at[pl.ds(0, 1)], one.at[1], me, hops=2)
    wo_g = ZThenY(wo, wo_f, wo_b, wo_yf, wo_yb, one.at[pl.ds(2, 1)], one.at[3], me, hops=2)
    gu = ZThenY(wgu, gu_f, gu_b, gu_yf, gu_yb, one.at[pl.ds(4, 2)], one.at[6], me, split=6)
    dn = YThenZ(wd, wd_y, wd_f, wd_b, one.at[7], me)
    ag1 = Gather(tall, ag1_s, one.at[8], one.at[9], me)
    ag2 = Gather(first, ag2_s, one.at[10], one.at[11], me)
    rs1 = Scatter(part1, other1, total1, via1, got1, rs1_s, one.at[12], me)
    rs2 = Scatter(part2, other2, total2, via2, got2, rs2_s, one.at[13], me)

    uv.z(0)
    uv.ys(0)
    wo_g.z(0)
    wo_g.ys(0)
    ag1.start()
    gu.z(0)
    gu.ys(0)
    dn.y0()
    everyone(me, gains, gain_s, one.at[14])

    uv.z(1)
    uv.z(2)
    uv.ys(1)
    uv.ys(2)
    wo_g.z(1)
    wo_g.z(2)
    wo_g.ys(1)
    wo_g.ys(2)
    uv.yf(0)
    wo_g.yf(0)
    gu.yf(0)
    gu.z(1)
    gu.ys(1)
    dn.y1()
    ag1.forward()

    uv.z(3)
    uv.z(4)
    uv.ys(3)
    uv.ys(4)
    wo_g.z(3)
    wo_g.z(4)
    wo_g.ys(3)
    wo_g.ys(4)
    dn.y2()
    dn.z(0)
    uv.yf(1)
    uv.yf(2)
    wo_g.yf(1)
    wo_g.yf(2)
    ag1.middle()
    gu.z(2)

    uv.z(5)
    uv.z(6)
    uv.ys(5)
    uv.ys(6)
    wo_g.z(5)
    wo_g.z(6)
    wo_g.ys(5)
    wo_g.ys(6)
    uv.yf(3)
    uv.yf(4)
    wo_g.yf(3)
    wo_g.yf(4)
    gu.yf(1)
    gu.ys(2)
    ag1.end()
    dn.z(1)

    uv.z(7)
    uv.z(8)
    uv.ys(7)
    uv.ys(8)
    wo_g.z(7)
    wo_g.z(8)
    wo_g.ys(7)
    wo_g.ys(8)
    uv.yf(5)
    uv.yf(6)
    wo_g.yf(5)
    wo_g.yf(6)
    gu.z(3)
    uv.yf(7)
    uv.yf(8)
    wo_g.yf(7)
    wo_g.yf(8)
    gu.yf(2)
    gu.ys(3)
    dn.z(2)
    ag1.finish()
    uv.finish()

    pre = jnp.dot(
        jnp.concatenate([tall[k] for k in range(8)], axis=1), wuv[...], preferred_element_type=F32
    )
    gated[...] = jax.nn.gelu(pre[:, 0:128])
    val = jax.nn.gelu(pre[:, 128:256])
    valued[...] = val
    stat1[me.t] = jnp.concatenate([row_sums(val), row_sums(val * val)], axis=0)
    everyone(me, stat1, st1_s, one.at[15])
    gu.z(4)
    gu.ys(4)
    gu.yf(3)
    from_everyone(me, stat1, st1_s)
    sums = jnp.sum(stat1[...], axis=0)
    mean = sums[0:1] / 1024.0
    rstd = lax.rsqrt(sums[1:2] / 1024.0 - mean * mean + EPS)
    normed = ((valued[...] - spread(mean)) * spread(rstd) * sgg[...]).astype(BF)
    keep = lax.broadcasted_iota(jnp.int32, (128, 128), 0) >= lax.broadcasted_iota(jnp.int32, (128, 128), 1)
    mask = jnp.where(keep, sw[0].astype(F32), 0.0).astype(BF)
    bias = spread(sb[...])
    wide = jnp.concatenate([normed[k * 128 : (k + 1) * 128] for k in range(4)], axis=1)
    mixed = jnp.dot(mask, wide, preferred_element_type=F32)
    for k in range(4):
        span = slice(k * 128, (k + 1) * 128)
        mixed_in[span, :] = (gated[span, :] * (mixed[:, span] + bias)).astype(BF)
    wo_g.finish()
    for d in (2, 1, 3, 0):
        xb = wrap(me.x + d, XN)
        left = mixed_in[pl.ds(pl.multiple_of(xb * 128, 128), 128), :]
        part1[pl.ds(xb * 2, 2)] = nt_dot(left, wo[...]).astype(BF).reshape(2, 64, 2048)
        rs1.swap(d)
    dn.z(3)
    rs1.far()
    rs1.near()
    gu.z(5)
    gu.ys(5)
    gu.yf(4)
    rs1.hop()
    dn.z(4)
    gu.z(6)
    gu.ys(6)
    gu.yf(5)
    mix = rs1.result()

    mine = pl.ds(pl.multiple_of(me.t * 64, 64), 64)
    held = jnp.concatenate([tall[k, mine, :] for k in range(8)], axis=1).astype(F32)
    resid = ALPHA * held + mix
    from_everyone(me, gains, gain_s)
    gain = jnp.concatenate([gains[k] for k in range(8)], axis=1)
    mean = jnp.sum(resid, axis=1, keepdims=True) / 2048.0
    square = jnp.sum(resid * resid, axis=1, keepdims=True) / 2048.0
    first[me.t] = ((resid - mean) * lax.rsqrt(square - mean * mean + EPS) * gain).astype(BF)
    ag2.start()
    dn.z(5)
    gu.z(7)
    gu.ys(7)
    gu.yf(6)
    ag2.forward()
    dn.z(6)
    ag2.middle()
    gu.z(8)
    gu.ys(8)
    gu.yf(7)
    ag2.end()
    dn.z(7)
    gu.yf(8)
    ag2.finish()
    gu.finish()

    pairs = [wrap(lax.div(me.z, 2) + j, 8) * 256 for j in (-2, -1, 0, 1, 2, 3, 4, 5)]
    spans = [pl.ds(pl.multiple_of(p, 256), 256) for p in pairs]

    def chunk(spans, cols):
        left = jnp.concatenate([first[:, :, span].reshape(512, 256) for span in spans], axis=1)
        right = jnp.concatenate([wgu[span, cols] for span in spans], axis=0)
        return jnp.dot(left, right, preferred_element_type=F32)

    for n in range(5):
        sums_in[:, n * 256 : (n + 1) * 256] = chunk(spans[:5], slice(n * 256, (n + 1) * 256))
    gu.finish_rest()
    for n in range(5):
        cols = slice(n * 256, (n + 1) * 256)
        acc = sums_in[:, cols] + chunk(spans[5:], cols)
        hidden[:, n * 128 : (n + 1) * 128] = (jax.nn.silu(acc[:, 0:128]) * acc[:, 128:256]).astype(BF)
    dn.z(8)
    acc = jnp.dot(first[...].reshape(512, 2048), wd[:, 768:896], preferred_element_type=F32)
    prod = jax.nn.silu(acc) * pltpu.roll(acc, 64, axis=1)
    real = lax.broadcasted_iota(jnp.int32, (512, 128), 1) < 64
    hidden[:, 640:768] = jnp.where(real, prod, 0.0).astype(BF)
    for d in (2, 1, 3, 0):
        xb = wrap(me.x + d, XN)
        for b in (xb * 2 + 1 - me.c, xb * 2 + me.c):
            cols = wd[pl.ds(pl.multiple_of(b * 256, 256), 256), 0:768]
            part2[b] = nt_dot(hidden[...], cols).astype(BF)
        rs2.swap(d)
        if d == 3:
            rs2.far()
    rs2.near()
    rs2.hop()
    ffn = rs2.result()

    here = pl.ds(pl.multiple_of(me.t * 256, 256), 256)
    second = ALPHA * first[:, :, here].reshape(512, 256).astype(F32) + ffn
    stat2[me.t] = jnp.concatenate([row_sums(second), row_sums(second * second)], axis=0)
    everyone(me, stat2, st2_s, one.at[16])
    from_everyone(me, stat2, st2_s)
    sums = jnp.sum(stat2[...], axis=0)
    mean = sums[0:1] / 2048.0
    rstd = lax.rsqrt(sums[1:2] / 2048.0 - mean * mean + EPS)
    mean, rstd = spread(mean), spread(rstd)
    for k in range(2):
        span = slice(k * 128, (k + 1) * 128)
        out[:, span] = ((second[:, span] - mean) * rstd * g2[:, span]).astype(BF)

    for each in (uv, wo_g, gu, dn, ag1, ag2, rs1, rs2):
        each.drain()
    drain_everyone(me, gains, one.at[14])
    drain_everyone(me, stat1, one.at[15])
    drain_everyone(me, stat2, one.at[16])


def on_device(tokens, u, v, sgg, sw, sb, ow, g1, gw, uw, dw, g2):
    vmem = pltpu.VMEM
    dma = pltpu.SemaphoreType.DMA
    scatter1 = [vmem((8, 64, 2048), BF), vmem((4, 64, 2048), BF), vmem((4, 64, 2048), BF), vmem((2, 32, 2048), BF), vmem((2, 64, 2048), BF)]
    scatter2 = [vmem((8, 512, 256), BF), vmem((4, 512, 256), BF), vmem((4, 512, 256), BF), vmem((2, 256, 256), BF), vmem((2, 512, 256), BF)]
    scratch = [
        vmem((2048, 256), BF), vmem((2048, 128), BF), vmem((2048, 1280), BF), vmem((2048, 896), BF),
        vmem((8, 512, 256), BF), vmem((8, 64, 2048), BF), vmem((8, 1, 256), F32), vmem((8, 2, 512), F32), vmem((8, 2, 512), F32),
        *scatter1, *scatter2,
        vmem((512, 128), F32), vmem((512, 128), F32), vmem((512, 128), BF), vmem((512, 1280), F32), vmem((512, 768), BF),
        vmem((1, 128), F32), vmem((1, 128, 128), BF), vmem((1, 128), F32),
        vmem((32, 704), BF), vmem((32, 704), BF), vmem((32, 704), BF), vmem((1, 256), F32),
        *[dma((9,)) for _ in range(12)],
        dma((4,)), dma((18,)), dma((18,)),
        dma((6,)), dma((6,)), dma((10,)), dma((10,)), dma((8,)), dma((8,)), dma((8,)), dma((17,)), dma((12,)),
    ]
    return pl.pallas_call(
        kernel,
        out_shape=jax.ShapeDtypeStruct((512, 256), BF),
        in_specs=[pl.BlockSpec(memory_space=pl.ANY)] * 12,
        out_specs=pl.BlockSpec(memory_space=pltpu.VMEM),
        scratch_shapes=scratch,
        compiler_params=pltpu.CompilerParams(collective_id=0, has_side_effects=True, vmem_limit_bytes=60 * 1024 * 1024),
    )(tokens, u, v, sgg.reshape(1, -1), sw, sb, ow.T, g1.reshape(1, -1), gw, uw, dw.T, g2.reshape(1, -1))


def solution(mesh):
    fs_tp, tp = P("fs", "tp"), P("tp")
    return jax.shard_map(
        on_device,
        mesh=mesh,
        in_specs=(
            fs_tp, fs_tp, fs_tp, tp, P("tp", None, None), P("tp", None), P("tp", "fs"), tp, fs_tp, fs_tp, P("tp", "fs"), tp,
        ),
        out_specs=fs_tp,
        check_vma=False,
    )
```

```python
import jax
import jax.numpy as jnp
from jax import lax
from jax.experimental import pallas as pl
from jax.experimental.pallas import tpu as pltpu
from jax.sharding import PartitionSpec as P

EPS = 1e-05
ALPHA = 2.0**0.25
MESH = pl.DeviceIdType.MESH
ZN, YN, XN = 16, 4, 4
BF, F32 = jnp.bfloat16, jnp.float32
UV_DIRECT, WO_DIRECT = 7, 7
ORDER = (
    ("ag1", "start"), ("wo", "z", 0), ("uv", "z", 0), ("dn", "y0"), ("gu", "z", 0), ("wo", "ys", 0), ("gu", "ys", 0),
    ("uv", "ys", 0), ("wo", "z", 1), ("dn", "y1"), ("uv", "z", 1), ("wo", "z", 2), ("uv", "z", 2), ("wo", "yf", 0),
    ("uv", "ys", 1), ("uv", "ys", 2), ("gu", "z", 1), ("wo", "z", 3), ("dn", "y2"), ("gu", "ys", 1), ("uv", "z", 3),
    ("wo", "z", 4), ("uv", "z", 4), ("dn", "z", 0, 0), ("uv", "ys", 3), ("uv", "ys", 4), ("wo", "ys", 1),
    ("ag1", "forward"), ("uv", "yf", 0), ("uv", "yf", 1), ("uv", "yf", 2), ("gu", "z", 2), ("wo", "ys", 2),
    ("wo", "ys", 3), ("wo", "ys", 4), ("uv", "z", 5), ("wo", "z", 5), ("wo", "z", 6), ("uv", "z", 6), ("wo", "ys", 5),
    ("uv", "ys", 5), ("uv", "ys", 6), ("gu", "ys", 2), ("dn", "z", 0, 1), ("wo", "z", 7), ("wo", "ys", 6),
    ("uv", "yf", 3), ("uv", "yf", 4), ("wo", "yf", 1), ("wo", "yf", 2), ("uv", "z", 7), ("ag1", "middle"),
    ("uv", "yf", 5), ("gu", "z", 3), ("dn", "z", 1, 0), ("uv", "ys", 7), ("uv", "z", 8), ("wo", "yf", 3),
    ("wo", "yf", 4), ("gu", "z", 4), ("uv", "ys", 8), ("ag1", "end"), ("ag1", "finish"), ("uv", "yf", 6),
    ("dn", "z", 1, 1), ("dn", "z", 2, 0), ("gu", "yf", 0), ("wo", "z", 8), ("wo", "ys", 7), ("wo", "ys", 8),
    ("gu", "ys", 3), ("gu", "z", 5), ("wo", "yf", 5), ("wo", "yf", 6), ("branches",), ("gu", "ys", 4),
    ("gu", "ys", 5), ("dn", "z", 2, 1), ("dn", "z", 3, 0), ("gu", "z", 6), ("gu", "yf", 1), ("gate",), ("rs1", "far"),
    ("dn", "z", 3, 1), ("gu", "ys", 6), ("dn", "z", 4, 0), ("gu", "yf", 2), ("gu", "yf", 3), ("gu", "yf", 4),
    ("rs1", "near"), ("rs1", "hop"), ("dn", "z", 4, 1), ("dn", "z", 5, 0), ("gu", "yf", 5), ("gu", "z", 7),
    ("gu", "ys", 7), ("dn", "z", 5, 1), ("gu", "yf", 6), ("norm_one",), ("dn", "z", 6, 0), ("gu", "z", 8),
    ("gu", "ys", 8), ("ag2", "forward"), ("dn", "z", 6, 1), ("dn", "z", 7, 0), ("ag2", "middle"), ("gu", "yf", 7),
    ("gu", "yf", 8), ("dn", "z", 7, 1), ("ag2", "end"), ("ag2", "finish"), ("near",), ("far",), ("dn", "z", 8, 0),
    ("dn", "z", 8, 1), ("down",), ("norm_two",),
)


def wrap(value, size):
    return lax.rem(value + size, size)


def nt_dot(left, right, **kw):
    return lax.dot_general(left, right, (((1,), (1,)), ((), ())), preferred_element_type=F32, **kw)


class Place:
    def __init__(self):
        f, t = lax.axis_index("fs"), lax.axis_index("tp")
        self.f, self.t = f, t
        self.z, self.y = lax.div(f, YN), lax.rem(f, YN)
        self.x, self.c = lax.div(t, 2), lax.rem(t, 2)
        self.zp = (wrap(self.z + 1, ZN) * YN + self.y, t)
        self.zm = (wrap(self.z - 1, ZN) * YN + self.y, t)
        self.yp = (self.z * YN + wrap(self.y + 1, YN), t)
        self.ym = (self.z * YN + wrap(self.y - 1, YN), t)
        self.y2 = (self.z * YN + wrap(self.y + 2, YN), t)
        self.xp = (f, wrap(self.x + 1, XN) * 2 + self.c)
        self.xm = (f, wrap(self.x - 1, XN) * 2 + self.c)
        self.mate = (f, self.x * 2 + 1 - self.c)

    def along_z(self, n):
        return (wrap(self.z + n, ZN) * YN + self.y, self.t)


def copy_to(src, dst, send, recv, dev):
    pltpu.make_async_remote_copy(src_ref=src, dst_ref=dst, send_sem=send, recv_sem=recv, device_id=dev, device_id_type=MESH).start()


def await_recv(dst, recv, dev):
    pltpu.make_async_remote_copy(src_ref=dst, dst_ref=dst, send_sem=recv, recv_sem=recv, device_id=dev, device_id_type=MESH).wait_recv()


def await_send(src, send, dev):
    pltpu.make_async_remote_copy(src_ref=src, dst_ref=src, send_sem=send, recv_sem=send, device_id=dev, device_id_type=MESH).wait_send()


class ZThenY:
    def __init__(self, w, f_sem, b_sem, yf_sem, yb_sem, last, sent, me, hops=1, split=9, direct=9):
        self.w, self.f_sem, self.b_sem, self.yf_sem, self.yb_sem = w, f_sem, b_sem, yf_sem, yb_sem
        self.last, self.sent, self.me, self.hops, self.split, self.direct = last, sent, me, hops, split, direct

    def block(self, zb, yb):
        row = (wrap(zb, ZN) * YN + wrap(yb, YN)) * 32
        return self.w.at[pl.ds(pl.multiple_of(row, 32), 32), :]

    def final(self, s):
        return self.last.at[0 if s < self.split else 1]

    def z(self, s):
        me = self.me
        fwd, bwd = self.block(me.z - s, me.y), self.block(me.z + s, me.y)
        steps = range(1, self.hops + 1) if s == 0 else (self.hops,)
        if s > 0:
            await_recv(fwd, self.f_sem.at[s], me.zm)
        for n in steps:
            if s + n <= 8:
                copy_to(fwd, fwd, self.sent, self.f_sem.at[s + n], me.along_z(n))
        if 0 < s < 8:
            await_recv(bwd, self.b_sem.at[s], me.zp)
        for n in steps:
            if s + n <= 7:
                copy_to(bwd, bwd, self.sent, self.b_sem.at[s + n], me.along_z(-n))

    def up(self, s, block):
        me = self.me
        copy_to(block, block, self.sent, self.yf_sem.at[s], me.yp)
        copy_to(block, block, self.sent, self.final(s), me.ym)

    def down(self, s, block):
        me = self.me
        copy_to(block, block, self.sent, self.yb_sem.at[s], me.ym)
        copy_to(block, block, self.sent, self.final(s), me.yp)

    def ys(self, s):
        me = self.me
        if s >= self.direct:
            for zb in (me.z - s, me.z + s)[: 1 if s in (0, 8) else 2]:
                block = self.block(zb, me.y)
                for dev in (me.yp, me.ym, me.y2):
                    copy_to(block, block, self.sent, self.final(s), dev)
            return
        if s < 8:
            self.up(s, self.block(me.z - s, me.y))
        if s > 0:
            self.down(s, self.block(me.z + s, me.y))

    def yf(self, s):
        me = self.me
        if s < 8:
            block = self.block(me.z - s, me.y - 1)
            await_recv(block, self.yf_sem.at[s], me.ym)
            copy_to(block, block, self.sent, self.final(s), me.yp)
        if s > 0:
            block = self.block(me.z + s, me.y + 1)
            await_recv(block, self.yb_sem.at[s], me.yp)
            copy_to(block, block, self.sent, self.final(s), me.ym)

    def finish(self, part=0):
        total = 0
        for s in range(9):
            if (s >= self.split) == (part == 1):
                total += (1 if s in (0, 8) else 2) * (3 if s >= self.direct else 2)
        await_recv(self.w.at[pl.ds(0, total * 32), :], self.last.at[part], self.me.yp)

    def drain(self):
        await_send(self.w.at[pl.ds(0, 2016), :], self.sent, self.me.yp)


class YThenZ:
    def __init__(self, w, y_sem, f_sem, b_sem, sent, me):
        self.w, self.y_sem, self.f_sem, self.b_sem, self.sent, self.me = w, y_sem, f_sem, b_sem, sent, me

    def rows(self, yb, start, size):
        row = (self.me.z * YN + wrap(yb, YN)) * 32 + start
        return self.w.at[pl.ds(pl.multiple_of(row, 16), size), :]

    def block(self, zb, h):
        return self.w.at[pl.ds(pl.multiple_of(wrap(zb, ZN) * 128 + h * 64, 64), 64), :]

    def y0(self):
        me = self.me
        own = self.rows(me.y, 0, 32)
        copy_to(own, own, self.sent, self.y_sem.at[0], me.yp)
        copy_to(own, own, self.sent, self.y_sem.at[1], me.ym)

    def y1(self):
        me = self.me
        await_recv(self.rows(me.y - 1, 0, 32), self.y_sem.at[0], me.ym)
        half = self.rows(me.y - 1, 0, 16)
        copy_to(half, half, self.sent, self.y_sem.at[2], me.yp)
        await_recv(self.rows(me.y + 1, 0, 32), self.y_sem.at[1], me.yp)
        half = self.rows(me.y + 1, 16, 16)
        copy_to(half, half, self.sent, self.y_sem.at[3], me.ym)

    def y2(self):
        me = self.me
        await_recv(self.rows(me.y - 2, 0, 16), self.y_sem.at[2], me.ym)
        await_recv(self.rows(me.y + 2, 16, 16), self.y_sem.at[3], me.yp)

    def z(self, s, h):
        me = self.me
        fwd, bwd = self.block(me.z - s, h), self.block(me.z + s, h)
        if 0 < s < 8 or (s == 8 and h == 0):
            await_recv(fwd, self.f_sem.at[h * 9 + s], me.zm)
        if s < 7 or (s == 7 and h == 0):
            copy_to(fwd, fwd, self.sent, self.f_sem.at[h * 9 + s + 1], me.zp)
        if 0 < s < 8 or (s == 8 and h == 1):
            await_recv(bwd, self.b_sem.at[h * 9 + s], me.zp)
        if s < 7 or (s == 7 and h == 1):
            copy_to(bwd, bwd, self.sent, self.b_sem.at[h * 9 + s + 1], me.zm)

    def drain(self):
        await_send(self.w.at[pl.ds(0, 2016), :], self.sent, self.me.yp)


class Gather:
    def __init__(self, buf, sem, relayed, sent, me):
        self.buf, self.sem, self.relayed, self.sent, self.me = buf, sem, relayed, sent, me
        self.half = buf.shape[1] // 2

    def part(self, xb, h):
        b = wrap(xb, XN) * 2 + self.me.c
        return self.buf.at[b, pl.ds(h * self.half, self.half), :]

    def send(self, xb, h, sem, dev):
        part = self.part(xb, h)
        copy_to(part, part, self.sent, sem, dev)

    def take(self, xb, h, sem, dev):
        await_recv(self.part(xb, h), sem, dev)

    def start(self):
        me = self.me
        self.send(me.x, 0, self.sem.at[0], me.xp)
        self.send(me.x, 1, self.sem.at[3], me.xm)
        self.send(me.x, 1, self.sem.at[1], me.xp)
        self.send(me.x, 0, self.sem.at[2], me.xm)
        own = self.buf.at[me.t]
        copy_to(own, own, self.sent, self.relayed, me.mate)

    def forward(self):
        me = self.me
        self.take(me.x - 1, 0, self.sem.at[0], me.xm)
        self.send(me.x - 1, 0, self.sem.at[4], me.xp)
        self.send(me.x - 1, 0, self.relayed, me.mate)
        self.take(me.x + 1, 1, self.sem.at[3], me.xp)
        self.send(me.x + 1, 1, self.sem.at[5], me.xm)
        self.send(me.x + 1, 1, self.relayed, me.mate)

    def middle(self):
        me = self.me
        self.take(me.x - 1, 1, self.sem.at[1], me.xm)
        self.send(me.x - 1, 1, self.relayed, me.mate)
        self.take(me.x + 1, 0, self.sem.at[2], me.xp)
        self.send(me.x + 1, 0, self.relayed, me.mate)

    def end(self):
        me = self.me
        self.take(me.x - 2, 0, self.sem.at[4], me.xm)
        self.send(me.x - 2, 0, self.relayed, me.mate)
        self.take(me.x + 2, 1, self.sem.at[5], me.xp)
        self.send(me.x + 2, 1, self.relayed, me.mate)

    def finish(self):
        await_recv(self.buf.at[pl.ds(0, 4)], self.relayed, self.me.mate)

    def drain(self):
        await_send(self.buf.at[pl.ds(0, 7)], self.sent, self.me.mate)


class Scatter:
    def __init__(self, part, other, total, via, got, sem, sent, me):
        self.part, self.other, self.total, self.via, self.got = part, other, total, via, got
        self.sem, self.sent, self.me = sem, sent, me
        self.half = part.shape[1] // 2

    def swap(self, d):
        me = self.me
        xb = wrap(me.x + d, XN)
        copy_to(self.part.at[xb * 2 + 1 - me.c], self.other.at[d], self.sent, self.sem.at[d], me.mate)

    def add(self, d):
        me = self.me
        xb = wrap(me.x + d, XN)
        await_recv(self.other.at[d], self.sem.at[d], me.mate)
        return self.part[xb * 2 + me.c].astype(F32) + self.other[d].astype(F32)

    def rows(self, h):
        return pl.ds(h * self.half, self.half)

    def far(self):
        me = self.me
        self.total[2] = self.add(2).astype(BF)
        copy_to(self.total.at[2, self.rows(0), :], self.via.at[0], self.sent, self.sem.at[4], me.xp)
        copy_to(self.total.at[2, self.rows(1), :], self.via.at[1], self.sent, self.sem.at[5], me.xm)

    def near(self):
        me = self.me
        self.total[1] = self.add(1).astype(BF)
        copy_to(self.total.at[1, self.rows(1), :], self.got.at[0, self.rows(1), :], self.sent, self.sem.at[6], me.xp)
        self.total[3] = self.add(3).astype(BF)
        copy_to(self.total.at[3, self.rows(0), :], self.got.at[1, self.rows(0), :], self.sent, self.sem.at[7], me.xm)

    def hop(self):
        me = self.me
        await_recv(self.via.at[0], self.sem.at[4], me.xm)
        self.total[1, self.rows(0), :] = (self.total[1, self.rows(0), :].astype(F32) + self.via[0].astype(F32)).astype(BF)
        copy_to(self.total.at[1, self.rows(0), :], self.got.at[0, self.rows(0), :], self.sent, self.sem.at[8], me.xp)
        await_recv(self.via.at[1], self.sem.at[5], me.xp)
        self.total[3, self.rows(1), :] = (self.total[3, self.rows(1), :].astype(F32) + self.via[1].astype(F32)).astype(BF)
        copy_to(self.total.at[3, self.rows(1), :], self.got.at[1, self.rows(1), :], self.sent, self.sem.at[9], me.xm)

    def result(self):
        me = self.me
        own = self.add(0)
        await_recv(self.got.at[0, self.rows(1), :], self.sem.at[6], me.xm)
        await_recv(self.got.at[1, self.rows(0), :], self.sem.at[7], me.xp)
        await_recv(self.got.at[0, self.rows(0), :], self.sem.at[8], me.xm)
        await_recv(self.got.at[1, self.rows(1), :], self.sem.at[9], me.xp)
        return (own + self.got[0].astype(F32) + self.got[1].astype(F32)).astype(BF).astype(F32)

    def drain(self):
        await_send(self.part.at[pl.ds(0, 7)], self.sent, self.me.mate)


def everyone(me, buf, recv, sent):
    own = buf.at[me.t]
    for d in range(1, 8):
        copy_to(own, own, sent, recv.at[d], (me.f, wrap(me.t + d, 8)))


def from_everyone(me, buf, recv):
    for d in range(1, 8):
        t = wrap(me.t - d, 8)
        await_recv(buf.at[t], recv.at[d], (me.f, t))


def drain_everyone(me, buf, sent):
    await_send(buf.at[pl.ds(0, 7)], sent, (me.f, wrap(me.t + 1, 8)))


def row_sums(vals):
    ones = jnp.ones((8, vals.shape[1]), F32)
    return nt_dot(ones, vals, precision=lax.Precision.HIGHEST)[0:1]


def spread(line, rows=128):
    return jnp.broadcast_to(line, (rows, line.shape[1])).T


def kernel(
    tok, u, v, sgg_in, sw_in, sb_in, ow, g1, gw_in, uw_in, dw_in, g2_in, out,
    wuv, wo, wgu, wd, tall, first, gains, stat1, stat2,
    part1, other1, total1, via1, got1, part2, other2, total2, via2, got2,
    gated, valued, mixed_in, sums_in, hidden, sgg, sw, sb, gw, uw, dw, g2,
    uv_f, uv_b, uv_yf, uv_yb, wo_f, wo_b, wo_yf, wo_yb, gu_f, gu_b, gu_yf, gu_yb, wd_y, wd_f, wd_b,
    ag1_s, ag2_s, rs1_s, rs2_s, gain_s, st1_s, st2_s, one, in_s,
):
    me = Place()
    barrier = pltpu.get_barrier_semaphore()
    for dev in (me.zp, me.zm, me.along_z(2), me.along_z(-2), me.yp, me.ym, me.y2):
        pl.semaphore_signal(barrier, inc=1, device_id=dev, device_id_type=MESH)
    for d in range(1, 8):
        pl.semaphore_signal(barrier, inc=1, device_id=(me.f, wrap(me.t + d, 8)), device_id_type=MESH)

    rows = pl.ds(pl.multiple_of(me.f * 32, 32), 32)
    loads = [
        pltpu.make_async_copy(src, dst, in_s.at[k])
        for k, (src, dst) in enumerate(
            (
                (u, wuv.at[rows, pl.ds(0, 128)]), (v, wuv.at[rows, pl.ds(128, 128)]), (ow, wo.at[rows, :]),
                (tok, tall.at[me.t]), (g1, gains.at[me.t]), (gw_in, gw), (uw_in, uw), (dw_in, dw),
                (sgg_in, sgg), (sw_in, sw), (sb_in, sb), (g2_in, g2),
            )
        )
    ]
    for load in loads:
        load.start()
    lane = lax.broadcasted_iota(jnp.int32, (64, 128), 1)
    line = lax.broadcasted_iota(jnp.int32, (64, 128), 0)
    low, high = (lane == line).astype(BF), (lane == line + 64).astype(BF)
    for load in loads:
        load.wait()
    for n in range(5):
        wgu[rows, n * 256 : n * 256 + 128] = gw[:, n * 128 : (n + 1) * 128]
        wgu[rows, n * 256 + 128 : n * 256 + 256] = uw[:, n * 128 : (n + 1) * 128]
    tail = jnp.dot(gw[:, 640:704], low, preferred_element_type=F32) + jnp.dot(uw[:, 640:704], high, preferred_element_type=F32)
    wd[rows, 768:896] = tail.astype(BF)
    wd[rows, 640:768] = jnp.zeros((32, 128), BF)
    wd[rows, 0:704] = dw[...]
    pl.semaphore_wait(barrier, 14)

    uv = ZThenY(wuv, uv_f, uv_b, uv_yf, uv_yb, one.at[pl.ds(0, 1)], one.at[1], me, hops=2, direct=UV_DIRECT)
    wo_g = ZThenY(wo, wo_f, wo_b, wo_yf, wo_yb, one.at[pl.ds(2, 1)], one.at[3], me, hops=2, direct=WO_DIRECT)
    gu = ZThenY(wgu, gu_f, gu_b, gu_yf, gu_yb, one.at[pl.ds(4, 2)], one.at[6], me, split=6)
    dn = YThenZ(wd, wd_y, wd_f, wd_b, one.at[7], me)
    ag1 = Gather(tall, ag1_s, one.at[8], one.at[9], me)
    ag2 = Gather(first, ag2_s, one.at[10], one.at[11], me)
    rs1 = Scatter(part1, other1, total1, via1, got1, rs1_s, one.at[12], me)
    rs2 = Scatter(part2, other2, total2, via2, got2, rs2_s, one.at[13], me)
    pairs = [wrap(lax.div(me.z, 2) + j, 8) * 256 for j in (-2, -1, 0, 1, 2, 3, 4, 5)]
    spans = [pl.ds(pl.multiple_of(p, 256), 256) for p in pairs]

    def branches():
        uv.finish()
        pre = jnp.dot(
            jnp.concatenate([tall[k] for k in range(8)], axis=1), wuv[...], preferred_element_type=F32
        )
        gated[...] = jax.nn.gelu(pre[:, 0:128])
        val = jax.nn.gelu(pre[:, 128:256])
        valued[...] = val
        stat1[me.t] = jnp.concatenate([row_sums(val), row_sums(val * val)], axis=0)
        everyone(me, stat1, st1_s, one.at[15])

    def gate():
        from_everyone(me, stat1, st1_s)
        sums = jnp.sum(stat1[...], axis=0)
        mean = sums[0:1] / 1024.0
        rstd = lax.rsqrt(sums[1:2] / 1024.0 - mean * mean + EPS)
        normed = ((valued[...] - spread(mean)) * spread(rstd) * sgg[...]).astype(BF)
        keep = lax.broadcasted_iota(jnp.int32, (128, 128), 0) >= lax.broadcasted_iota(jnp.int32, (128, 128), 1)
        mask = jnp.where(keep, sw[0].astype(F32), 0.0).astype(BF)
        bias = spread(sb[...])
        wide = jnp.concatenate([normed[k * 128 : (k + 1) * 128] for k in range(4)], axis=1)
        mixed = jnp.dot(mask, wide, preferred_element_type=F32)
        for k in range(4):
            span = slice(k * 128, (k + 1) * 128)
            mixed_in[span, :] = (gated[span, :] * (mixed[:, span] + bias)).astype(BF)
        wo_g.finish()
        for d in (2, 1, 3, 0):
            xb = wrap(me.x + d, XN)
            left = mixed_in[pl.ds(pl.multiple_of(xb * 128, 128), 128), :]
            part1[pl.ds(xb * 2, 2)] = nt_dot(left, wo[...]).astype(BF).reshape(2, 64, 2048)
            rs1.swap(d)

    def norm_one():
        mine = pl.ds(pl.multiple_of(me.t * 64, 64), 64)
        held = jnp.concatenate([tall[k, mine, :] for k in range(8)], axis=1).astype(F32)
        resid = ALPHA * held + rs1.result()
        from_everyone(me, gains, gain_s)
        gain = jnp.concatenate([gains[k] for k in range(8)], axis=1)
        mean = jnp.sum(resid, axis=1, keepdims=True) / 2048.0
        square = jnp.sum(resid * resid, axis=1, keepdims=True) / 2048.0
        first[me.t] = ((resid - mean) * lax.rsqrt(square - mean * mean + EPS) * gain).astype(BF)
        ag2.start()

    def chunk(spans, cols):
        left = jnp.concatenate([first[:, :, span].reshape(512, 256) for span in spans], axis=1)
        right = jnp.concatenate([wgu[span, cols] for span in spans], axis=0)
        return jnp.dot(left, right, preferred_element_type=F32)

    def hidden_near():
        gu.finish()
        for n in range(5):
            sums_in[:, n * 256 : (n + 1) * 256] = chunk(spans[:5], slice(n * 256, (n + 1) * 256))

    def hidden_far():
        gu.finish(1)
        for n in range(5):
            cols = slice(n * 256, (n + 1) * 256)
            acc = sums_in[:, cols] + chunk(spans[5:], cols)
            hidden[:, n * 128 : (n + 1) * 128] = (jax.nn.silu(acc[:, 0:128]) * acc[:, 128:256]).astype(BF)

    def down():
        acc = jnp.dot(first[...].reshape(512, 2048), wd[:, 768:896], preferred_element_type=F32)
        prod = jax.nn.silu(acc) * pltpu.roll(acc, 64, axis=1)
        real = lax.broadcasted_iota(jnp.int32, (512, 128), 1) < 64
        hidden[:, 640:768] = jnp.where(real, prod, 0.0).astype(BF)
        for d in (2, 1, 3, 0):
            xb = wrap(me.x + d, XN)
            for b in (xb * 2 + 1 - me.c, xb * 2 + me.c):
                cols = wd[pl.ds(pl.multiple_of(b * 256, 256), 256), 0:768]
                part2[b] = nt_dot(hidden[...], cols).astype(BF)
            rs2.swap(d)
            if d == 3:
                rs2.far()
        rs2.near()
        rs2.hop()

    def norm_two():
        here = pl.ds(pl.multiple_of(me.t * 256, 256), 256)
        second = ALPHA * first[:, :, here].reshape(512, 256).astype(F32) + rs2.result()
        stat2[me.t] = jnp.concatenate([row_sums(second), row_sums(second * second)], axis=0)
        everyone(me, stat2, st2_s, one.at[16])
        from_everyone(me, stat2, st2_s)
        sums = jnp.sum(stat2[...], axis=0)
        mean = sums[0:1] / 2048.0
        rstd = lax.rsqrt(sums[1:2] / 2048.0 - mean * mean + EPS)
        mean, rstd = spread(mean), spread(rstd)
        for k in range(2):
            span = slice(k * 128, (k + 1) * 128)
            out[:, span] = ((second[:, span] - mean) * rstd * g2[:, span]).astype(BF)

    parts = {
        "uv": uv, "wo": wo_g, "gu": gu, "dn": dn, "ag1": ag1, "ag2": ag2, "rs1": rs1,
        "branches": branches, "gate": gate, "norm_one": norm_one, "near": hidden_near,
        "far": hidden_far, "down": down, "norm_two": norm_two,
    }

    def act(name, method=None, *at):
        part = parts[name]
        (part if method is None else getattr(part, method))(*at)

    everyone(me, gains, gain_s, one.at[14])
    for step in ORDER:
        act(*step)

    for each in (uv, wo_g, gu, dn, ag1, ag2, rs1, rs2):
        each.drain()
    drain_everyone(me, gains, one.at[14])
    drain_everyone(me, stat1, one.at[15])
    drain_everyone(me, stat2, one.at[16])


def on_device(tokens, u, v, sgg, sw, sb, ow, g1, gw, uw, dw, g2):
    vmem = pltpu.VMEM
    dma = pltpu.SemaphoreType.DMA
    scatter1 = [vmem((8, 64, 2048), BF), vmem((4, 64, 2048), BF), vmem((4, 64, 2048), BF), vmem((2, 32, 2048), BF), vmem((2, 64, 2048), BF)]
    scatter2 = [vmem((8, 512, 256), BF), vmem((4, 512, 256), BF), vmem((4, 512, 256), BF), vmem((2, 256, 256), BF), vmem((2, 512, 256), BF)]
    scratch = [
        vmem((2048, 256), BF), vmem((2048, 128), BF), vmem((2048, 1280), BF), vmem((2048, 896), BF),
        vmem((8, 512, 256), BF), vmem((8, 64, 2048), BF), vmem((8, 1, 256), F32), vmem((8, 2, 512), F32), vmem((8, 2, 512), F32),
        *scatter1, *scatter2,
        vmem((512, 128), F32), vmem((512, 128), F32), vmem((512, 128), BF), vmem((512, 1280), F32), vmem((512, 768), BF),
        vmem((1, 128), F32), vmem((1, 128, 128), BF), vmem((1, 128), F32),
        vmem((32, 704), BF), vmem((32, 704), BF), vmem((32, 704), BF), vmem((1, 256), F32),
        *[dma((9,)) for _ in range(12)],
        dma((4,)), dma((18,)), dma((18,)),
        dma((6,)), dma((6,)), dma((10,)), dma((10,)), dma((8,)), dma((8,)), dma((8,)), dma((17,)), dma((12,)),
    ]
    return pl.pallas_call(
        kernel,
        out_shape=jax.ShapeDtypeStruct((512, 256), BF),
        in_specs=[pl.BlockSpec(memory_space=pl.ANY)] * 12,
        out_specs=pl.BlockSpec(memory_space=pltpu.VMEM),
        scratch_shapes=scratch,
        compiler_params=pltpu.CompilerParams(collective_id=0, has_side_effects=True, vmem_limit_bytes=60 * 1024 * 1024),
    )(tokens, u, v, sgg.reshape(1, -1), sw, sb, ow.T, g1.reshape(1, -1), gw, uw, dw.T, g2.reshape(1, -1))


def solution(mesh):
    fs_tp, tp = P("fs", "tp"), P("tp")
    return jax.shard_map(
        on_device,
        mesh=mesh,
        in_specs=(
            fs_tp, fs_tp, fs_tp, tp, P("tp", None, None), P("tp", None), P("tp", "fs"), tp, fs_tp, fs_tp, P("tp", "fs"), tp,
        ),
        out_specs=fs_tp,
        check_vma=False,
    )
```

```python
import jax
import jax.numpy as jnp
from jax import lax
from jax.experimental import pallas as pl
from jax.experimental.pallas import tpu as pltpu
from jax.sharding import PartitionSpec as P

EPS = 1e-05
ALPHA = 2.0**0.25
MESH = pl.DeviceIdType.MESH
ZN, YN, XN = 16, 4, 4
BF, F32 = jnp.bfloat16, jnp.float32
UV_DIRECT, WO_DIRECT, UV_HOPS, WO_HOPS = 7, 9, 2, 1
ORDER = (
    ("ag1", "start"), ("wo", "z", 0), ("uv", "z", 0), ("uv", "ys", 0), ("pack",), ("gu", "z", 0), ("dn", "y0"),
    ("gu", "ys", 0), ("wo", "z", 1), ("uv", "z", 1), ("wo", "ys", 0), ("dn", "y1"), ("uv", "z", 2), ("uv", "ys", 1),
    ("uv", "yf", 0), ("wo", "z", 2), ("wo", "ys", 1), ("wo", "ys", 2), ("uv", "ys", 2), ("gu", "z", 1),
    ("uv", "z", 3), ("gu", "ys", 1), ("wo", "z", 3), ("uv", "z", 4), ("dn", "y2"), ("dn", "z", 0, 0), ("wo", "z", 4),
    ("ag1", "forward"), ("ag1", "middle"), ("wo", "ys", 3), ("wo", "ys", 4), ("uv", "yf", 1), ("uv", "yf", 2),
    ("wo", "yf", 0), ("uv", "z", 5), ("gu", "z", 2), ("uv", "z", 6), ("uv", "ys", 3), ("uv", "ys", 4),
    ("uv", "ys", 5), ("uv", "ys", 6), ("wo", "z", 5), ("dn", "z", 0, 1), ("gu", "ys", 2), ("gu", "z", 3),
    ("wo", "z", 6), ("uv", "z", 7), ("uv", "yf", 3), ("dn", "z", 1, 0), ("uv", "z", 8), ("uv", "yf", 4),
    ("uv", "yf", 5), ("uv", "ys", 7), ("wo", "ys", 5), ("wo", "z", 7), ("gu", "z", 4), ("uv", "ys", 8),
    ("ag1", "end"), ("wo", "ys", 6), ("wo", "yf", 1), ("uv", "yf", 6), ("dn", "z", 1, 1), ("wo", "ys", 7),
    ("wo", "yf", 2), ("wo", "yf", 3), ("wo", "yf", 4), ("wo", "yf", 5), ("ag1", "finish"), ("wo", "z", 8),
    ("wo", "ys", 8), ("dn", "z", 2, 0), ("gu", "ys", 3), ("branches",), ("gu", "z", 5), ("wo", "yf", 6),
    ("wo", "yf", 7), ("dn", "z", 2, 1), ("wo", "yf", 8), ("gu", "ys", 4), ("gu", "ys", 5), ("gu", "yf", 0),
    ("dn", "z", 3, 0), ("gate",), ("gu", "z", 6), ("rs1", "far"), ("rs1", "near"), ("gu", "ys", 6), ("gu", "yf", 1),
    ("dn", "z", 3, 1), ("dn", "z", 4, 0), ("rs1", "hop"), ("gu", "z", 7), ("gu", "yf", 2), ("gu", "ys", 7),
    ("dn", "z", 4, 1), ("dn", "z", 5, 0), ("gu", "yf", 3), ("gu", "yf", 4), ("norm_one",), ("gu", "z", 8),
    ("gu", "yf", 5), ("dn", "z", 5, 1), ("dn", "z", 6, 0), ("gu", "ys", 8), ("ag2", "forward"), ("dn", "z", 6, 1),
    ("gu", "yf", 6), ("gu", "yf", 7), ("ag2", "middle"), ("gu", "yf", 8), ("dn", "z", 7, 0), ("dn", "z", 7, 1),
    ("ag2", "end"), ("ag2", "finish"), ("near",), ("dn", "z", 8, 0), ("far",), ("dn", "z", 8, 1), ("down",),
    ("norm_two",),
)


def wrap(value, size):
    return lax.rem(value + size, size)


def nt_dot(left, right, **kw):
    return lax.dot_general(left, right, (((1,), (1,)), ((), ())), preferred_element_type=F32, **kw)


class Place:
    def __init__(self):
        f, t = lax.axis_index("fs"), lax.axis_index("tp")
        self.f, self.t = f, t
        self.z, self.y = lax.div(f, YN), lax.rem(f, YN)
        self.x, self.c = lax.div(t, 2), lax.rem(t, 2)
        self.zp = (wrap(self.z + 1, ZN) * YN + self.y, t)
        self.zm = (wrap(self.z - 1, ZN) * YN + self.y, t)
        self.yp = (self.z * YN + wrap(self.y + 1, YN), t)
        self.ym = (self.z * YN + wrap(self.y - 1, YN), t)
        self.y2 = (self.z * YN + wrap(self.y + 2, YN), t)
        self.xp = (f, wrap(self.x + 1, XN) * 2 + self.c)
        self.xm = (f, wrap(self.x - 1, XN) * 2 + self.c)
        self.mate = (f, self.x * 2 + 1 - self.c)

    def along_z(self, n):
        return (wrap(self.z + n, ZN) * YN + self.y, self.t)


def copy_to(src, dst, send, recv, dev):
    pltpu.make_async_remote_copy(src_ref=src, dst_ref=dst, send_sem=send, recv_sem=recv, device_id=dev, device_id_type=MESH).start()


def await_recv(dst, recv, dev):
    pltpu.make_async_remote_copy(src_ref=dst, dst_ref=dst, send_sem=recv, recv_sem=recv, device_id=dev, device_id_type=MESH).wait_recv()


def await_send(src, send, dev):
    pltpu.make_async_remote_copy(src_ref=src, dst_ref=src, send_sem=send, recv_sem=send, device_id=dev, device_id_type=MESH).wait_send()


class ZThenY:
    def __init__(self, w, f_sem, b_sem, yf_sem, yb_sem, last, sent, me, hops=1, split=9, direct=9):
        self.w, self.f_sem, self.b_sem, self.yf_sem, self.yb_sem = w, f_sem, b_sem, yf_sem, yb_sem
        self.last, self.sent, self.me, self.hops, self.split, self.direct = last, sent, me, hops, split, direct

    def block(self, zb, yb):
        row = (wrap(zb, ZN) * YN + wrap(yb, YN)) * 32
        return self.w.at[pl.ds(pl.multiple_of(row, 32), 32), :]

    def side(self, block, s, h):
        return block.at[pl.ds(h * 16, 16), :] if s == 8 else block

    def final(self, s):
        return self.last.at[0 if s < self.split else 1]

    def z(self, s):
        me = self.me
        fwd, bwd = self.block(me.z - s, me.y), self.block(me.z + s, me.y)
        steps = range(1, self.hops + 1) if s == 0 else (self.hops,)
        if s > 0:
            await_recv(self.side(fwd, s, 0), self.f_sem.at[s], me.zm)
        for n in steps:
            if s + n <= 8:
                part = self.side(fwd, s + n, 0)
                copy_to(part, part, self.sent, self.f_sem.at[s + n], me.along_z(n))
        if s > 0:
            await_recv(self.side(bwd, s, 1), self.b_sem.at[s], me.zp)
        for n in steps:
            if s + n <= 8:
                part = self.side(bwd, s + n, 1)
                copy_to(part, part, self.sent, self.b_sem.at[s + n], me.along_z(-n))

    def up(self, s, block):
        me = self.me
        copy_to(block, block, self.sent, self.yf_sem.at[s], me.yp)
        copy_to(block, block, self.sent, self.final(s), me.ym)

    def down(self, s, block):
        me = self.me
        copy_to(block, block, self.sent, self.yb_sem.at[s], me.ym)
        copy_to(block, block, self.sent, self.final(s), me.yp)

    def ys(self, s):
        me = self.me
        if s >= self.direct:
            for zb in (me.z - s, me.z + s)[: 1 if s in (0, 8) else 2]:
                block = self.block(zb, me.y)
                for dev in (me.yp, me.ym, me.y2):
                    copy_to(block, block, self.sent, self.final(s), dev)
            return
        if s < 8:
            self.up(s, self.block(me.z - s, me.y))
        if s > 0:
            self.down(s, self.block(me.z + s, me.y))

    def yf(self, s):
        me = self.me
        if s < 8:
            block = self.block(me.z - s, me.y - 1)
            await_recv(block, self.yf_sem.at[s], me.ym)
            copy_to(block, block, self.sent, self.final(s), me.yp)
        if s > 0:
            block = self.block(me.z + s, me.y + 1)
            await_recv(block, self.yb_sem.at[s], me.yp)
            copy_to(block, block, self.sent, self.final(s), me.ym)

    def finish(self, part=0):
        total = 0
        for s in range(9):
            if (s >= self.split) == (part == 1):
                total += (1 if s in (0, 8) else 2) * (3 if s >= self.direct else 2)
        await_recv(self.w.at[pl.ds(0, total * 32), :], self.last.at[part], self.me.yp)

    def drain(self):
        await_send(self.w.at[pl.ds(0, 2016), :], self.sent, self.me.yp)


class YThenZ:
    def __init__(self, w, y_sem, f_sem, b_sem, sent, me):
        self.w, self.y_sem, self.f_sem, self.b_sem, self.sent, self.me = w, y_sem, f_sem, b_sem, sent, me

    def rows(self, yb, start, size):
        row = (self.me.z * YN + wrap(yb, YN)) * 32 + start
        return self.w.at[pl.ds(pl.multiple_of(row, 16), size), :]

    def block(self, zb, h):
        return self.w.at[pl.ds(pl.multiple_of(wrap(zb, ZN) * 128 + h * 64, 64), 64), :]

    def y0(self):
        me = self.me
        own = self.rows(me.y, 0, 32)
        copy_to(own, own, self.sent, self.y_sem.at[0], me.yp)
        copy_to(own, own, self.sent, self.y_sem.at[1], me.ym)

    def y1(self):
        me = self.me
        await_recv(self.rows(me.y - 1, 0, 32), self.y_sem.at[0], me.ym)
        half = self.rows(me.y - 1, 0, 16)
        copy_to(half, half, self.sent, self.y_sem.at[2], me.yp)
        await_recv(self.rows(me.y + 1, 0, 32), self.y_sem.at[1], me.yp)
        half = self.rows(me.y + 1, 16, 16)
        copy_to(half, half, self.sent, self.y_sem.at[3], me.ym)

    def y2(self):
        me = self.me
        await_recv(self.rows(me.y - 2, 0, 16), self.y_sem.at[2], me.ym)
        await_recv(self.rows(me.y + 2, 16, 16), self.y_sem.at[3], me.yp)

    def z(self, s, h):
        me = self.me
        fwd, bwd = self.block(me.z - s, h), self.block(me.z + s, h)
        if 0 < s < 8 or (s == 8 and h == 0):
            await_recv(fwd, self.f_sem.at[h * 9 + s], me.zm)
        if s < 7 or (s == 7 and h == 0):
            copy_to(fwd, fwd, self.sent, self.f_sem.at[h * 9 + s + 1], me.zp)
        if 0 < s < 8 or (s == 8 and h == 1):
            await_recv(bwd, self.b_sem.at[h * 9 + s], me.zp)
        if s < 7 or (s == 7 and h == 1):
            copy_to(bwd, bwd, self.sent, self.b_sem.at[h * 9 + s + 1], me.zm)

    def drain(self):
        await_send(self.w.at[pl.ds(0, 2016), :], self.sent, self.me.yp)


class Gather:
    def __init__(self, buf, sem, relayed, sent, me):
        self.buf, self.sem, self.relayed, self.sent, self.me = buf, sem, relayed, sent, me
        self.half = buf.shape[1] // 2

    def part(self, xb, h):
        b = wrap(xb, XN) * 2 + self.me.c
        return self.buf.at[b, pl.ds(h * self.half, self.half), :]

    def send(self, xb, h, sem, dev):
        part = self.part(xb, h)
        copy_to(part, part, self.sent, sem, dev)

    def take(self, xb, h, sem, dev):
        await_recv(self.part(xb, h), sem, dev)

    def start(self):
        me = self.me
        self.send(me.x, 0, self.sem.at[0], me.xp)
        self.send(me.x, 1, self.sem.at[3], me.xm)
        self.send(me.x, 1, self.sem.at[1], me.xp)
        self.send(me.x, 0, self.sem.at[2], me.xm)
        own = self.buf.at[me.t]
        copy_to(own, own, self.sent, self.relayed, me.mate)

    def forward(self):
        me = self.me
        self.take(me.x - 1, 0, self.sem.at[0], me.xm)
        self.send(me.x - 1, 0, self.sem.at[4], me.xp)
        self.send(me.x - 1, 0, self.relayed, me.mate)
        self.take(me.x + 1, 1, self.sem.at[3], me.xp)
        self.send(me.x + 1, 1, self.sem.at[5], me.xm)
        self.send(me.x + 1, 1, self.relayed, me.mate)

    def middle(self):
        me = self.me
        self.take(me.x - 1, 1, self.sem.at[1], me.xm)
        self.send(me.x - 1, 1, self.relayed, me.mate)
        self.take(me.x + 1, 0, self.sem.at[2], me.xp)
        self.send(me.x + 1, 0, self.relayed, me.mate)

    def end(self):
        me = self.me
        self.take(me.x - 2, 0, self.sem.at[4], me.xm)
        self.send(me.x - 2, 0, self.relayed, me.mate)
        self.take(me.x + 2, 1, self.sem.at[5], me.xp)
        self.send(me.x + 2, 1, self.relayed, me.mate)

    def finish(self):
        await_recv(self.buf.at[pl.ds(0, 4)], self.relayed, self.me.mate)

    def drain(self):
        await_send(self.buf.at[pl.ds(0, 7)], self.sent, self.me.mate)


class Scatter:
    def __init__(self, part, other, total, via, got, sem, sent, me):
        self.part, self.other, self.total, self.via, self.got = part, other, total, via, got
        self.sem, self.sent, self.me = sem, sent, me
        self.half = part.shape[1] // 2

    def swap(self, d):
        me = self.me
        xb = wrap(me.x + d, XN)
        copy_to(self.part.at[xb * 2 + 1 - me.c], self.other.at[d], self.sent, self.sem.at[d], me.mate)

    def add(self, d):
        me = self.me
        xb = wrap(me.x + d, XN)
        await_recv(self.other.at[d], self.sem.at[d], me.mate)
        return self.part[xb * 2 + me.c].astype(F32) + self.other[d].astype(F32)

    def rows(self, h):
        return pl.ds(h * self.half, self.half)

    def far(self):
        me = self.me
        self.total[2] = self.add(2).astype(BF)
        copy_to(self.total.at[2, self.rows(0), :], self.via.at[0], self.sent, self.sem.at[4], me.xp)
        copy_to(self.total.at[2, self.rows(1), :], self.via.at[1], self.sent, self.sem.at[5], me.xm)

    def near(self):
        me = self.me
        self.total[1] = self.add(1).astype(BF)
        copy_to(self.total.at[1, self.rows(1), :], self.got.at[0, self.rows(1), :], self.sent, self.sem.at[6], me.xp)
        self.total[3] = self.add(3).astype(BF)
        copy_to(self.total.at[3, self.rows(0), :], self.got.at[1, self.rows(0), :], self.sent, self.sem.at[7], me.xm)

    def hop(self):
        me = self.me
        await_recv(self.via.at[0], self.sem.at[4], me.xm)
        self.total[1, self.rows(0), :] = (self.total[1, self.rows(0), :].astype(F32) + self.via[0].astype(F32)).astype(BF)
        copy_to(self.total.at[1, self.rows(0), :], self.got.at[0, self.rows(0), :], self.sent, self.sem.at[8], me.xp)
        await_recv(self.via.at[1], self.sem.at[5], me.xp)
        self.total[3, self.rows(1), :] = (self.total[3, self.rows(1), :].astype(F32) + self.via[1].astype(F32)).astype(BF)
        copy_to(self.total.at[3, self.rows(1), :], self.got.at[1, self.rows(1), :], self.sent, self.sem.at[9], me.xm)

    def result(self):
        me = self.me
        own = self.add(0)
        await_recv(self.got.at[0, self.rows(1), :], self.sem.at[6], me.xm)
        await_recv(self.got.at[1, self.rows(0), :], self.sem.at[7], me.xp)
        await_recv(self.got.at[0, self.rows(0), :], self.sem.at[8], me.xm)
        await_recv(self.got.at[1, self.rows(1), :], self.sem.at[9], me.xp)
        return (own + self.got[0].astype(F32) + self.got[1].astype(F32)).astype(BF).astype(F32)

    def drain(self):
        await_send(self.part.at[pl.ds(0, 7)], self.sent, self.me.mate)


def everyone(me, buf, recv, sent):
    own = buf.at[me.t]
    for d in range(1, 8):
        copy_to(own, own, sent, recv.at[d], (me.f, wrap(me.t + d, 8)))


def from_everyone(me, buf, recv):
    for d in range(1, 8):
        t = wrap(me.t - d, 8)
        await_recv(buf.at[t], recv.at[d], (me.f, t))


def drain_everyone(me, buf, sent):
    await_send(buf.at[pl.ds(0, 7)], sent, (me.f, wrap(me.t + 1, 8)))


def row_sums(vals):
    ones = jnp.ones((8, vals.shape[1]), F32)
    return nt_dot(ones, vals, precision=lax.Precision.HIGHEST)[0:1]


def spread(line, rows=128):
    return jnp.broadcast_to(line, (rows, line.shape[1])).T


def kernel(
    tok, u, v, sgg_in, sw_in, sb_in, ow, g1, gw_in, uw_in, dw_in, g2_in, out,
    wuv, wo, wgu, wd, tall, first, gains, stat1, stat2,
    part1, other1, total1, via1, got1, part2, other2, total2, via2, got2,
    gated, valued, mixed_in, sums_in, hidden, sgg, sw, sb, gw, uw, dw, g2,
    uv_f, uv_b, uv_yf, uv_yb, wo_f, wo_b, wo_yf, wo_yb, gu_f, gu_b, gu_yf, gu_yb, wd_y, wd_f, wd_b,
    ag1_s, ag2_s, rs1_s, rs2_s, gain_s, st1_s, st2_s, one, in_s,
):
    me = Place()
    barrier = pltpu.get_barrier_semaphore()
    for dev in (me.zp, me.zm, me.along_z(2), me.along_z(-2), me.yp, me.ym, me.y2):
        pl.semaphore_signal(barrier, inc=1, device_id=dev, device_id_type=MESH)
    for d in range(1, 8):
        pl.semaphore_signal(barrier, inc=1, device_id=(me.f, wrap(me.t + d, 8)), device_id_type=MESH)

    rows = pl.ds(pl.multiple_of(me.f * 32, 32), 32)
    loads = [
        pltpu.make_async_copy(src, dst, in_s.at[k])
        for k, (src, dst) in enumerate(
            (
                (u, wuv.at[rows, pl.ds(0, 128)]), (v, wuv.at[rows, pl.ds(128, 128)]), (ow, wo.at[rows, :]),
                (tok, tall.at[me.t]), (g1, gains.at[me.t]), (gw_in, gw), (uw_in, uw), (dw_in, dw),
                (sgg_in, sgg), (sw_in, sw), (sb_in, sb), (g2_in, g2),
            )
        )
    ]
    for load in loads:
        load.start()
    for load in loads[:5]:
        load.wait()
    pl.semaphore_wait(barrier, 14)

    uv = ZThenY(wuv, uv_f, uv_b, uv_yf, uv_yb, one.at[pl.ds(0, 1)], one.at[1], me, hops=UV_HOPS, direct=UV_DIRECT)
    wo_g = ZThenY(wo, wo_f, wo_b, wo_yf, wo_yb, one.at[pl.ds(2, 1)], one.at[3], me, hops=WO_HOPS, direct=WO_DIRECT)
    gu = ZThenY(wgu, gu_f, gu_b, gu_yf, gu_yb, one.at[pl.ds(4, 2)], one.at[6], me, split=6)
    dn = YThenZ(wd, wd_y, wd_f, wd_b, one.at[7], me)
    ag1 = Gather(tall, ag1_s, one.at[8], one.at[9], me)
    ag2 = Gather(first, ag2_s, one.at[10], one.at[11], me)
    rs1 = Scatter(part1, other1, total1, via1, got1, rs1_s, one.at[12], me)
    rs2 = Scatter(part2, other2, total2, via2, got2, rs2_s, one.at[13], me)
    pairs = [wrap(lax.div(me.z, 2) + j, 8) * 256 for j in (-2, -1, 0, 1, 2, 3, 4, 5)]
    spans = [pl.ds(pl.multiple_of(p, 256), 256) for p in pairs]

    def pack():
        for load in loads[5:]:
            load.wait()
        lane = lax.broadcasted_iota(jnp.int32, (64, 128), 1)
        line = lax.broadcasted_iota(jnp.int32, (64, 128), 0)
        low, high = (lane == line).astype(BF), (lane == line + 64).astype(BF)
        for n in range(5):
            wgu[rows, n * 256 : n * 256 + 128] = gw[:, n * 128 : (n + 1) * 128]
            wgu[rows, n * 256 + 128 : n * 256 + 256] = uw[:, n * 128 : (n + 1) * 128]
        tail = jnp.dot(gw[:, 640:704], low, preferred_element_type=F32) + jnp.dot(uw[:, 640:704], high, preferred_element_type=F32)
        wd[rows, 768:896] = tail.astype(BF)
        wd[rows, 640:768] = jnp.zeros((32, 128), BF)
        wd[rows, 0:704] = dw[...]

    def branches():
        uv.finish()
        everyone(me, gains, gain_s, one.at[14])
        pre = jnp.dot(
            jnp.concatenate([tall[k] for k in range(8)], axis=1), wuv[...], preferred_element_type=F32
        )
        gated[...] = jax.nn.gelu(pre[:, 0:128])
        val = jax.nn.gelu(pre[:, 128:256])
        valued[...] = val
        stat1[me.t] = jnp.concatenate([row_sums(val), row_sums(val * val)], axis=0)
        everyone(me, stat1, st1_s, one.at[15])

    def gate():
        from_everyone(me, stat1, st1_s)
        sums = jnp.sum(stat1[...], axis=0)
        mean = sums[0:1] / 1024.0
        rstd = lax.rsqrt(sums[1:2] / 1024.0 - mean * mean + EPS)
        normed = ((valued[...] - spread(mean)) * spread(rstd) * sgg[...]).astype(BF)
        keep = lax.broadcasted_iota(jnp.int32, (128, 128), 0) >= lax.broadcasted_iota(jnp.int32, (128, 128), 1)
        mask = jnp.where(keep, sw[0].astype(F32), 0.0).astype(BF)
        bias = spread(sb[...])
        wide = jnp.concatenate([normed[k * 128 : (k + 1) * 128] for k in range(4)], axis=1)
        mixed = jnp.dot(mask, wide, preferred_element_type=F32)
        for k in range(4):
            span = slice(k * 128, (k + 1) * 128)
            mixed_in[span, :] = (gated[span, :] * (mixed[:, span] + bias)).astype(BF)
        wo_g.finish()
        for d in (2, 1, 3, 0):
            xb = wrap(me.x + d, XN)
            left = mixed_in[pl.ds(pl.multiple_of(xb * 128, 128), 128), :]
            part1[pl.ds(xb * 2, 2)] = nt_dot(left, wo[...]).astype(BF).reshape(2, 64, 2048)
            rs1.swap(d)

    def norm_one():
        mine = pl.ds(pl.multiple_of(me.t * 64, 64), 64)
        held = jnp.concatenate([tall[k, mine, :] for k in range(8)], axis=1).astype(F32)
        resid = ALPHA * held + rs1.result()
        from_everyone(me, gains, gain_s)
        gain = jnp.concatenate([gains[k] for k in range(8)], axis=1)
        mean = jnp.sum(resid, axis=1, keepdims=True) / 2048.0
        square = jnp.sum(resid * resid, axis=1, keepdims=True) / 2048.0
        first[me.t] = ((resid - mean) * lax.rsqrt(square - mean * mean + EPS) * gain).astype(BF)
        ag2.start()

    def chunk(spans, cols):
        left = jnp.concatenate([first[:, :, span].reshape(512, 256) for span in spans], axis=1)
        right = jnp.concatenate([wgu[span, cols] for span in spans], axis=0)
        return jnp.dot(left, right, preferred_element_type=F32)

    def hidden_near():
        gu.finish()
        for n in range(5):
            sums_in[:, n * 256 : (n + 1) * 256] = chunk(spans[:5], slice(n * 256, (n + 1) * 256))

    def hidden_far():
        gu.finish(1)
        for n in range(5):
            cols = slice(n * 256, (n + 1) * 256)
            acc = sums_in[:, cols] + chunk(spans[5:], cols)
            hidden[:, n * 128 : (n + 1) * 128] = (jax.nn.silu(acc[:, 0:128]) * acc[:, 128:256]).astype(BF)

    def down():
        acc = jnp.dot(first[...].reshape(512, 2048), wd[:, 768:896], preferred_element_type=F32)
        prod = jax.nn.silu(acc) * pltpu.roll(acc, 64, axis=1)
        real = lax.broadcasted_iota(jnp.int32, (512, 128), 1) < 64
        hidden[:, 640:768] = jnp.where(real, prod, 0.0).astype(BF)
        for d in (2, 1, 3, 0):
            xb = wrap(me.x + d, XN)
            for b in (xb * 2 + 1 - me.c, xb * 2 + me.c):
                cols = wd[pl.ds(pl.multiple_of(b * 256, 256), 256), 0:768]
                part2[b] = nt_dot(hidden[...], cols).astype(BF)
            rs2.swap(d)
            if d == 3:
                rs2.far()
        rs2.near()
        rs2.hop()

    def norm_two():
        here = pl.ds(pl.multiple_of(me.t * 256, 256), 256)
        second = ALPHA * first[:, :, here].reshape(512, 256).astype(F32) + rs2.result()
        stat2[me.t] = jnp.concatenate([row_sums(second), row_sums(second * second)], axis=0)
        everyone(me, stat2, st2_s, one.at[16])
        from_everyone(me, stat2, st2_s)
        sums = jnp.sum(stat2[...], axis=0)
        mean = sums[0:1] / 2048.0
        rstd = lax.rsqrt(sums[1:2] / 2048.0 - mean * mean + EPS)
        mean, rstd = spread(mean), spread(rstd)
        for k in range(2):
            span = slice(k * 128, (k + 1) * 128)
            out[:, span] = ((second[:, span] - mean) * rstd * g2[:, span]).astype(BF)

    parts = {
        "uv": uv, "wo": wo_g, "gu": gu, "dn": dn, "ag1": ag1, "ag2": ag2, "rs1": rs1,
        "pack": pack, "branches": branches, "gate": gate, "norm_one": norm_one, "near": hidden_near,
        "far": hidden_far, "down": down, "norm_two": norm_two,
    }

    def act(name, method=None, *at):
        part = parts[name]
        (part if method is None else getattr(part, method))(*at)

    for step in ORDER:
        act(*step)

    for each in (uv, wo_g, gu, dn, ag1, ag2, rs1, rs2):
        each.drain()
    drain_everyone(me, gains, one.at[14])
    drain_everyone(me, stat1, one.at[15])
    drain_everyone(me, stat2, one.at[16])


def on_device(tokens, u, v, sgg, sw, sb, ow, g1, gw, uw, dw, g2):
    vmem = pltpu.VMEM
    dma = pltpu.SemaphoreType.DMA
    scatter1 = [vmem((8, 64, 2048), BF), vmem((4, 64, 2048), BF), vmem((4, 64, 2048), BF), vmem((2, 32, 2048), BF), vmem((2, 64, 2048), BF)]
    scatter2 = [vmem((8, 512, 256), BF), vmem((4, 512, 256), BF), vmem((4, 512, 256), BF), vmem((2, 256, 256), BF), vmem((2, 512, 256), BF)]
    scratch = [
        vmem((2048, 256), BF), vmem((2048, 128), BF), vmem((2048, 1280), BF), vmem((2048, 896), BF),
        vmem((8, 512, 256), BF), vmem((8, 64, 2048), BF), vmem((8, 1, 256), F32), vmem((8, 2, 512), F32), vmem((8, 2, 512), F32),
        *scatter1, *scatter2,
        vmem((512, 128), F32), vmem((512, 128), F32), vmem((512, 128), BF), vmem((512, 1280), F32), vmem((512, 768), BF),
        vmem((1, 128), F32), vmem((1, 128, 128), BF), vmem((1, 128), F32),
        vmem((32, 704), BF), vmem((32, 704), BF), vmem((32, 704), BF), vmem((1, 256), F32),
        *[dma((9,)) for _ in range(12)],
        dma((4,)), dma((18,)), dma((18,)),
        dma((6,)), dma((6,)), dma((10,)), dma((10,)), dma((8,)), dma((8,)), dma((8,)), dma((17,)), dma((12,)),
    ]
    args = (tokens, u, v, sgg.reshape(1, -1), sw, sb, ow.T, g1.reshape(1, -1), gw, uw, dw.T, g2.reshape(1, -1))
    args = [pltpu.with_memory_space_constraint(a, pltpu.HBM) for a in args]
    return pl.pallas_call(
        kernel,
        out_shape=jax.ShapeDtypeStruct((512, 256), BF),
        in_specs=[pl.BlockSpec(memory_space=pltpu.HBM)] * 12,
        out_specs=pl.BlockSpec(memory_space=pltpu.VMEM),
        scratch_shapes=scratch,
        compiler_params=pltpu.CompilerParams(collective_id=0, has_side_effects=True, vmem_limit_bytes=40 * 1024 * 1024),
    )(*args)


def solution(mesh):
    fs_tp, tp = P("fs", "tp"), P("tp")
    return jax.shard_map(
        on_device,
        mesh=mesh,
        in_specs=(
            fs_tp, fs_tp, fs_tp, tp, P("tp", None, None), P("tp", None), P("tp", "fs"), tp, fs_tp, fs_tp, P("tp", "fs"), tp,
        ),
        out_specs=fs_tp,
        check_vma=False,
    )
```

```python
import jax
import jax.numpy as jnp
from jax import lax
from jax.experimental import pallas as pl
from jax.experimental.pallas import tpu as pltpu
from jax.sharding import PartitionSpec as P

EPS = 1e-05
ALPHA = 2.0**0.25
MESH = pl.DeviceIdType.MESH
ZN, YN, XN = 16, 4, 4
BF, F32 = jnp.bfloat16, jnp.float32
UV_DIRECT, WO_DIRECT, UV_HOPS, WO_HOPS = 9, 9, 2, 2
ORDER = (
    ("uv", "z", 0), ("ag1", "start"), ("wo", "z", 0), ("uv", "ys", 0), ("wo", "ys", 0), ("pack",), ("gu", "z", 0),
    ("dn", "y0"), ("gu", "ys", 0), ("uv", "z", 1), ("uv", "ys", 1), ("wo", "z", 1), ("uv", "z", 2), ("uv", "yf", 0),
    ("uv", "ys", 2), ("wo", "z", 2), ("wo", "ys", 1), ("wo", "ys", 2), ("dn", "y1"), ("ag1", "forward"),
    ("gu", "z", 1), ("gu", "ys", 1), ("wo", "z", 3), ("uv", "z", 3), ("uv", "z", 4), ("wo", "yf", 0), ("wo", "z", 4),
    ("gu", "z", 2), ("gu", "ys", 2), ("wo", "z", 5), ("uv", "ys", 3), ("uv", "z", 5), ("uv", "z", 6), ("dn", "y2"),
    ("wo", "yf", 1), ("wo", "z", 6), ("wo", "yf", 2), ("uv", "yf", 1), ("dn", "z", 0, 0), ("uv", "ys", 4),
    ("wo", "ys", 3), ("ag1", "middle"), ("ag1", "end"), ("uv", "ys", 5), ("gu", "z", 3), ("uv", "ys", 6),
    ("wo", "ys", 4), ("uv", "z", 7), ("wo", "z", 7), ("wo", "z", 8), ("dn", "z", 0, 1), ("uv", "ys", 7),
    ("uv", "z", 8), ("wo", "ys", 5), ("uv", "ys", 8), ("wo", "ys", 6), ("wo", "ys", 7), ("uv", "yf", 2),
    ("uv", "yf", 3), ("dn", "z", 1, 0), ("uv", "yf", 4), ("ag1", "finish"), ("uv", "yf", 5), ("wo", "ys", 8),
    ("uv", "yf", 6), ("uv", "yf", 7), ("uv", "yf", 8), ("gu", "ys", 3), ("gu", "z", 4), ("wo", "yf", 3),
    ("wo", "yf", 4), ("gu", "yf", 0), ("wo", "yf", 5), ("dn", "z", 1, 1), ("dn", "z", 2, 0), ("wo", "yf", 6),
    ("wo", "yf", 7), ("gu", "yf", 1), ("wo", "yf", 8), ("gu", "ys", 4), ("branches",), ("gu", "z", 5),
    ("gu", "ys", 5), ("dn", "z", 2, 1), ("dn", "z", 3, 0), ("gate",), ("gu", "yf", 2), ("rs1", "far"),
    ("rs1", "near"), ("gu", "z", 6), ("dn", "z", 3, 1), ("gu", "ys", 6), ("dn", "z", 4, 0), ("gu", "yf", 3),
    ("gu", "yf", 4), ("gu", "z", 7), ("rs1", "hop"), ("dn", "z", 4, 1), ("dn", "z", 5, 0), ("gu", "z", 8),
    ("gu", "ys", 7), ("gu", "yf", 5), ("norm_one",), ("gu", "ys", 8), ("dn", "z", 5, 1), ("dn", "z", 6, 0),
    ("ag2", "forward"), ("dn", "z", 6, 1), ("gu", "yf", 6), ("gu", "yf", 7), ("gu", "yf", 8), ("ag2", "middle"),
    ("dn", "z", 7, 0), ("ag2", "end"), ("dn", "z", 7, 1), ("ag2", "finish"), ("near",), ("dn", "z", 8, 0), ("far",),
    ("dn", "z", 8, 1), ("down",), ("norm_two",),
)


def wrap(value, size):
    return lax.rem(value + size, size)


def nt_dot(left, right, **kw):
    return lax.dot_general(left, right, (((1,), (1,)), ((), ())), preferred_element_type=F32, **kw)


class Place:
    def __init__(self):
        f, t = lax.axis_index("fs"), lax.axis_index("tp")
        self.f, self.t = f, t
        self.z, self.y = lax.div(f, YN), lax.rem(f, YN)
        self.x, self.c = lax.div(t, 2), lax.rem(t, 2)
        self.zp = (wrap(self.z + 1, ZN) * YN + self.y, t)
        self.zm = (wrap(self.z - 1, ZN) * YN + self.y, t)
        self.yp = (self.z * YN + wrap(self.y + 1, YN), t)
        self.ym = (self.z * YN + wrap(self.y - 1, YN), t)
        self.y2 = (self.z * YN + wrap(self.y + 2, YN), t)
        self.xp = (f, wrap(self.x + 1, XN) * 2 + self.c)
        self.xm = (f, wrap(self.x - 1, XN) * 2 + self.c)
        self.mate = (f, self.x * 2 + 1 - self.c)

    def along_z(self, n):
        return (wrap(self.z + n, ZN) * YN + self.y, self.t)


def copy_to(src, dst, send, recv, dev):
    pltpu.make_async_remote_copy(src_ref=src, dst_ref=dst, send_sem=send, recv_sem=recv, device_id=dev, device_id_type=MESH).start()


def await_recv(dst, recv, dev):
    pltpu.make_async_remote_copy(src_ref=dst, dst_ref=dst, send_sem=recv, recv_sem=recv, device_id=dev, device_id_type=MESH).wait_recv()


def await_send(src, send, dev):
    pltpu.make_async_remote_copy(src_ref=src, dst_ref=src, send_sem=send, recv_sem=send, device_id=dev, device_id_type=MESH).wait_send()


class ZThenY:
    def __init__(self, w, f_sem, b_sem, yf_sem, yb_sem, last, sent, me, hops=1, split=9, direct=9):
        self.w, self.f_sem, self.b_sem, self.yf_sem, self.yb_sem = w, f_sem, b_sem, yf_sem, yb_sem
        self.last, self.sent, self.me, self.hops, self.split, self.direct = last, sent, me, hops, split, direct

    def block(self, zb, yb):
        row = (wrap(zb, ZN) * YN + wrap(yb, YN)) * 32
        return self.w.at[pl.ds(pl.multiple_of(row, 32), 32), :]

    def side(self, block, s, h):
        return block.at[pl.ds(h * 16, 16), :] if s == 8 else block

    def final(self, s):
        return self.last.at[0 if s < self.split else 1]

    def z(self, s):
        me = self.me
        fwd, bwd = self.block(me.z - s, me.y), self.block(me.z + s, me.y)
        steps = range(1, self.hops + 1) if s == 0 else (self.hops,)
        if s > 0:
            await_recv(self.side(fwd, s, 0), self.f_sem.at[s], me.zm)
        for n in steps:
            if s + n <= 8:
                part = self.side(fwd, s + n, 0)
                copy_to(part, part, self.sent, self.f_sem.at[s + n], me.along_z(n))
        if s > 0:
            await_recv(self.side(bwd, s, 1), self.b_sem.at[s], me.zp)
        for n in steps:
            if s + n <= 8:
                part = self.side(bwd, s + n, 1)
                copy_to(part, part, self.sent, self.b_sem.at[s + n], me.along_z(-n))

    def up(self, s, block):
        me = self.me
        copy_to(block, block, self.sent, self.yf_sem.at[s], me.yp)
        copy_to(block, block, self.sent, self.final(s), me.ym)

    def down(self, s, block):
        me = self.me
        copy_to(block, block, self.sent, self.yb_sem.at[s], me.ym)
        copy_to(block, block, self.sent, self.final(s), me.yp)

    def ys(self, s):
        me = self.me
        if s >= self.direct:
            for zb in (me.z - s, me.z + s)[: 1 if s in (0, 8) else 2]:
                block = self.block(zb, me.y)
                for dev in (me.yp, me.ym, me.y2):
                    copy_to(block, block, self.sent, self.final(s), dev)
            return
        if s < 8:
            self.up(s, self.block(me.z - s, me.y))
        if s > 0:
            self.down(s, self.block(me.z + s, me.y))

    def yf(self, s):
        me = self.me
        if s < 8:
            block = self.block(me.z - s, me.y - 1)
            await_recv(block, self.yf_sem.at[s], me.ym)
            copy_to(block, block, self.sent, self.final(s), me.yp)
        if s > 0:
            block = self.block(me.z + s, me.y + 1)
            await_recv(block, self.yb_sem.at[s], me.yp)
            copy_to(block, block, self.sent, self.final(s), me.ym)

    def finish(self, part=0):
        total = 0
        for s in range(9):
            if (s >= self.split) == (part == 1):
                total += (1 if s in (0, 8) else 2) * (3 if s >= self.direct else 2)
        await_recv(self.w.at[pl.ds(0, total * 32), :], self.last.at[part], self.me.yp)

    def drain(self):
        await_send(self.w.at[pl.ds(0, 2016), :], self.sent, self.me.yp)


class YThenZ:
    def __init__(self, w, y_sem, f_sem, b_sem, sent, me):
        self.w, self.y_sem, self.f_sem, self.b_sem, self.sent, self.me = w, y_sem, f_sem, b_sem, sent, me

    def shard(self, yb, start=0, size=13):
        return self.w.at[self.me.z * YN + wrap(yb, YN), pl.ds(start, size)]

    def block(self, zb, h):
        return self.w.at[pl.ds(wrap(zb, ZN) * 4 + h * 2, 2)]

    def y0(self):
        me = self.me
        own = self.shard(me.y)
        copy_to(own, own, self.sent, self.y_sem.at[0], me.yp)
        copy_to(own, own, self.sent, self.y_sem.at[1], me.ym)

    def y1(self):
        me = self.me
        await_recv(self.shard(me.y - 1), self.y_sem.at[0], me.ym)
        half = self.shard(me.y - 1, 0, 7)
        copy_to(half, half, self.sent, self.y_sem.at[2], me.yp)
        await_recv(self.shard(me.y + 1), self.y_sem.at[1], me.yp)
        half = self.shard(me.y + 1, 7, 6)
        copy_to(half, half, self.sent, self.y_sem.at[3], me.ym)

    def y2(self):
        me = self.me
        await_recv(self.shard(me.y - 2, 0, 7), self.y_sem.at[2], me.ym)
        await_recv(self.shard(me.y + 2, 7, 6), self.y_sem.at[3], me.yp)

    def z(self, s, h):
        me = self.me
        fwd, bwd = self.block(me.z - s, h), self.block(me.z + s, h)
        if 0 < s < 8 or (s == 8 and h == 0):
            await_recv(fwd, self.f_sem.at[h * 9 + s], me.zm)
        if s < 7 or (s == 7 and h == 0):
            copy_to(fwd, fwd, self.sent, self.f_sem.at[h * 9 + s + 1], me.zp)
        if 0 < s < 8 or (s == 8 and h == 1):
            await_recv(bwd, self.b_sem.at[h * 9 + s], me.zp)
        if s < 7 or (s == 7 and h == 1):
            copy_to(bwd, bwd, self.sent, self.b_sem.at[h * 9 + s + 1], me.zm)

    def drain(self):
        await_send(self.w.at[pl.ds(0, 63)], self.sent, self.me.yp)


class Gather:
    def __init__(self, buf, sem, relayed, sent, me):
        self.buf, self.sem, self.relayed, self.sent, self.me = buf, sem, relayed, sent, me
        self.half = buf.shape[1] // 2

    def part(self, xb, h):
        b = wrap(xb, XN) * 2 + self.me.c
        return self.buf.at[b, pl.ds(h * self.half, self.half), :]

    def send(self, xb, h, sem, dev):
        part = self.part(xb, h)
        copy_to(part, part, self.sent, sem, dev)

    def take(self, xb, h, sem, dev):
        await_recv(self.part(xb, h), sem, dev)

    def start(self):
        me = self.me
        self.send(me.x, 0, self.sem.at[0], me.xp)
        self.send(me.x, 1, self.sem.at[3], me.xm)
        self.send(me.x, 1, self.sem.at[1], me.xp)
        self.send(me.x, 0, self.sem.at[2], me.xm)
        own = self.buf.at[me.t]
        copy_to(own, own, self.sent, self.relayed, me.mate)

    def forward(self):
        me = self.me
        self.take(me.x - 1, 0, self.sem.at[0], me.xm)
        self.send(me.x - 1, 0, self.sem.at[4], me.xp)
        self.send(me.x - 1, 0, self.relayed, me.mate)
        self.take(me.x + 1, 1, self.sem.at[3], me.xp)
        self.send(me.x + 1, 1, self.sem.at[5], me.xm)
        self.send(me.x + 1, 1, self.relayed, me.mate)

    def middle(self):
        me = self.me
        self.take(me.x - 1, 1, self.sem.at[1], me.xm)
        self.send(me.x - 1, 1, self.relayed, me.mate)
        self.take(me.x + 1, 0, self.sem.at[2], me.xp)
        self.send(me.x + 1, 0, self.relayed, me.mate)

    def end(self):
        me = self.me
        self.take(me.x - 2, 0, self.sem.at[4], me.xm)
        self.send(me.x - 2, 0, self.relayed, me.mate)
        self.take(me.x + 2, 1, self.sem.at[5], me.xp)
        self.send(me.x + 2, 1, self.relayed, me.mate)

    def finish(self):
        await_recv(self.buf.at[pl.ds(0, 4)], self.relayed, self.me.mate)

    def drain(self):
        await_send(self.buf.at[pl.ds(0, 7)], self.sent, self.me.mate)


class Scatter:
    def __init__(self, part, other, total, via, got, sem, sent, me):
        self.part, self.other, self.total, self.via, self.got = part, other, total, via, got
        self.sem, self.sent, self.me = sem, sent, me
        self.half = part.shape[1] // 2

    def swap(self, d):
        me = self.me
        xb = wrap(me.x + d, XN)
        copy_to(self.part.at[xb * 2 + 1 - me.c], self.other.at[d], self.sent, self.sem.at[d], me.mate)

    def add(self, d):
        me = self.me
        xb = wrap(me.x + d, XN)
        await_recv(self.other.at[d], self.sem.at[d], me.mate)
        return self.part[xb * 2 + me.c].astype(F32) + self.other[d].astype(F32)

    def rows(self, h):
        return pl.ds(h * self.half, self.half)

    def far(self):
        me = self.me
        self.total[2] = self.add(2).astype(BF)
        copy_to(self.total.at[2, self.rows(0), :], self.via.at[0], self.sent, self.sem.at[4], me.xp)
        copy_to(self.total.at[2, self.rows(1), :], self.via.at[1], self.sent, self.sem.at[5], me.xm)

    def near(self):
        me = self.me
        self.total[1] = self.add(1).astype(BF)
        copy_to(self.total.at[1, self.rows(1), :], self.got.at[0, self.rows(1), :], self.sent, self.sem.at[6], me.xp)
        self.total[3] = self.add(3).astype(BF)
        copy_to(self.total.at[3, self.rows(0), :], self.got.at[1, self.rows(0), :], self.sent, self.sem.at[7], me.xm)

    def hop(self):
        me = self.me
        await_recv(self.via.at[0], self.sem.at[4], me.xm)
        self.total[1, self.rows(0), :] = (self.total[1, self.rows(0), :].astype(F32) + self.via[0].astype(F32)).astype(BF)
        copy_to(self.total.at[1, self.rows(0), :], self.got.at[0, self.rows(0), :], self.sent, self.sem.at[8], me.xp)
        await_recv(self.via.at[1], self.sem.at[5], me.xp)
        self.total[3, self.rows(1), :] = (self.total[3, self.rows(1), :].astype(F32) + self.via[1].astype(F32)).astype(BF)
        copy_to(self.total.at[3, self.rows(1), :], self.got.at[1, self.rows(1), :], self.sent, self.sem.at[9], me.xm)

    def result(self):
        me = self.me
        own = self.add(0)
        await_recv(self.got.at[0, self.rows(1), :], self.sem.at[6], me.xm)
        await_recv(self.got.at[1, self.rows(0), :], self.sem.at[7], me.xp)
        await_recv(self.got.at[0, self.rows(0), :], self.sem.at[8], me.xm)
        await_recv(self.got.at[1, self.rows(1), :], self.sem.at[9], me.xp)
        return (own + self.got[0].astype(F32) + self.got[1].astype(F32)).astype(BF).astype(F32)

    def drain(self):
        await_send(self.part.at[pl.ds(0, 7)], self.sent, self.me.mate)


def everyone(me, buf, recv, sent):
    own = buf.at[me.t]
    for d in (4, 3, 5, 2, 6, 1, 7):
        copy_to(own, own, sent, recv.at[d], (me.f, wrap(me.t + d, 8)))


def from_everyone(me, buf, recv):
    for d in range(1, 8):
        t = wrap(me.t - d, 8)
        await_recv(buf.at[t], recv.at[d], (me.f, t))


def drain_everyone(me, buf, sent):
    await_send(buf.at[pl.ds(0, 7)], sent, (me.f, wrap(me.t + 1, 8)))


def row_sums(vals):
    folded = vals[:, 0:128]
    for k in range(1, vals.shape[1] // 128):
        folded = folded + vals[:, k * 128 : (k + 1) * 128]
    return jnp.sum(folded.T, axis=0, keepdims=True)


def spread(line, rows=128):
    return jnp.broadcast_to(line, (rows, line.shape[1])).T


def kernel(
    tok, u, v, sgg_in, sw_in, sb_in, ow, g1, gw_in, uw_in, dw_in, g2_in, out,
    wuv, wo, wgu, wd, tall, first, gains, stat1, stat2,
    part1, other1, total1, via1, got1, part2, other2, total2, via2, got2,
    gated, valued, mixed_in, sums_in, hidden, sgg, sw, sb, gw, uw, dw, g2,
    uv_f, uv_b, uv_yf, uv_yb, wo_f, wo_b, wo_yf, wo_yb, gu_f, gu_b, gu_yf, gu_yb, wd_y, wd_f, wd_b,
    ag1_s, ag2_s, rs1_s, rs2_s, gain_s, st1_s, st2_s, one, in_s,
):
    me = Place()
    barrier = pltpu.get_barrier_semaphore()
    for dev in (me.zp, me.zm, me.along_z(2), me.along_z(-2), me.yp, me.ym, me.y2):
        pl.semaphore_signal(barrier, inc=1, device_id=dev, device_id_type=MESH)
    for d in range(1, 8):
        pl.semaphore_signal(barrier, inc=1, device_id=(me.f, wrap(me.t + d, 8)), device_id_type=MESH)

    rows = pl.ds(pl.multiple_of(me.f * 32, 32), 32)
    loads = [
        pltpu.make_async_copy(src, dst, in_s.at[k])
        for k, (src, dst) in enumerate(
            (
                (u, wuv.at[rows, pl.ds(0, 128)]), (v, wuv.at[rows, pl.ds(128, 128)]), (ow, wo.at[rows, :]),
                (tok, tall.at[me.t]), (g1, gains.at[me.t]), (gw_in, gw), (uw_in, uw), (dw_in, dw),
                (sgg_in, sgg), (sw_in, sw), (sb_in, sb), (g2_in, g2),
            )
        )
    ]
    for load in loads:
        load.start()
    for load in loads[:3]:
        load.wait()
    pl.semaphore_wait(barrier, 14)

    uv = ZThenY(wuv, uv_f, uv_b, uv_yf, uv_yb, one.at[pl.ds(0, 1)], one.at[1], me, hops=UV_HOPS, direct=UV_DIRECT)
    wo_g = ZThenY(wo, wo_f, wo_b, wo_yf, wo_yb, one.at[pl.ds(2, 1)], one.at[3], me, hops=WO_HOPS, direct=WO_DIRECT)
    gu = ZThenY(wgu, gu_f, gu_b, gu_yf, gu_yb, one.at[pl.ds(4, 2)], one.at[6], me, split=6)
    dn = YThenZ(wd, wd_y, wd_f, wd_b, one.at[7], me)
    ag1 = Gather(tall, ag1_s, one.at[8], one.at[9], me)
    ag2 = Gather(first, ag2_s, one.at[10], one.at[11], me)
    rs1 = Scatter(part1, other1, total1, via1, got1, rs1_s, one.at[12], me)
    rs2 = Scatter(part2, other2, total2, via2, got2, rs2_s, one.at[13], me)
    pairs = [wrap(lax.div(me.z, 2) + j, 8) * 256 for j in (-2, -1, 0, 1, 2, 3, 4, 5)]
    spans = [pl.ds(pl.multiple_of(p, 256), 256) for p in pairs]

    def pack():
        for load in loads[4:]:
            load.wait()
        lane = lax.broadcasted_iota(jnp.int32, (64, 128), 1)
        line = lax.broadcasted_iota(jnp.int32, (64, 128), 0)
        low, high = (lane == line).astype(BF), (lane == line + 64).astype(BF)
        for n in range(5):
            wgu[rows, n * 256 : n * 256 + 128] = gw[:, n * 128 : (n + 1) * 128]
            wgu[rows, n * 256 + 128 : n * 256 + 256] = uw[:, n * 128 : (n + 1) * 128]
        tail = jnp.dot(gw[:, 640:704], low, preferred_element_type=F32) + jnp.dot(uw[:, 640:704], high, preferred_element_type=F32)
        wd[me.f, 11:13] = tail.astype(BF).reshape(2, 16, 128)
        for n in range(5):
            wd[me.f, 2 * n : 2 * n + 2] = dw[:, n * 128 : (n + 1) * 128].reshape(2, 16, 128)
        both = jnp.dot(dw[0:16, 640:704], low, preferred_element_type=F32) + jnp.dot(dw[16:32, 640:704], high, preferred_element_type=F32)
        wd[me.f, 10] = both.astype(BF)

    def branches():
        uv.finish()
        everyone(me, gains, gain_s, one.at[14])
        pre = jnp.dot(
            jnp.concatenate([tall[k] for k in range(8)], axis=1), wuv[...], preferred_element_type=F32
        )
        gated[...] = jax.nn.gelu(pre[:, 0:128])
        val = jax.nn.gelu(pre[:, 128:256])
        valued[...] = val
        stat1[me.t] = jnp.concatenate([row_sums(val), row_sums(val * val)], axis=0)
        everyone(me, stat1, st1_s, one.at[15])

    def gate():
        from_everyone(me, stat1, st1_s)
        sums = jnp.sum(stat1[...], axis=0)
        mean = sums[0:1] / 1024.0
        rstd = lax.rsqrt(sums[1:2] / 1024.0 - mean * mean + EPS)
        normed = ((valued[...] - spread(mean)) * spread(rstd) * sgg[...]).astype(BF)
        keep = lax.broadcasted_iota(jnp.int32, (128, 128), 0) >= lax.broadcasted_iota(jnp.int32, (128, 128), 1)
        mask = jnp.where(keep, sw[0].astype(F32), 0.0).astype(BF)
        bias = spread(sb[...])
        wide = jnp.concatenate([normed[k * 128 : (k + 1) * 128] for k in range(4)], axis=1)
        mixed = jnp.dot(mask, wide, preferred_element_type=F32)
        for k in range(4):
            span = slice(k * 128, (k + 1) * 128)
            mixed_in[span, :] = (gated[span, :] * (mixed[:, span] + bias)).astype(BF)
        wo_g.finish()
        for d in (2, 1, 3, 0):
            xb = wrap(me.x + d, XN)
            left = mixed_in[pl.ds(pl.multiple_of(xb * 128, 128), 128), :]
            part1[pl.ds(xb * 2, 2)] = nt_dot(left, wo[...]).astype(BF).reshape(2, 64, 2048)
            rs1.swap(d)

    def norm_one():
        mine = pl.ds(pl.multiple_of(me.t * 64, 64), 64)
        held = jnp.concatenate([tall[k, mine, :] for k in range(8)], axis=1).astype(F32)
        resid = ALPHA * held + rs1.result()
        from_everyone(me, gains, gain_s)
        gain = jnp.concatenate([gains[k] for k in range(8)], axis=1)
        mean = jnp.sum(resid, axis=1, keepdims=True) / 2048.0
        square = jnp.sum(resid * resid, axis=1, keepdims=True) / 2048.0
        first[me.t] = ((resid - mean) * lax.rsqrt(square - mean * mean + EPS) * gain).astype(BF)
        ag2.start()

    def chunk(spans, cols):
        left = jnp.concatenate([first[:, :, span].reshape(512, 256) for span in spans], axis=1)
        right = jnp.concatenate([wgu[span, cols] for span in spans], axis=0)
        return jnp.dot(left, right, preferred_element_type=F32)

    def hidden_near():
        gu.finish()
        for n in range(5):
            sums_in[:, n * 256 : (n + 1) * 256] = chunk(spans[:5], slice(n * 256, (n + 1) * 256))

    def hidden_far():
        gu.finish(1)
        for n in range(5):
            cols = slice(n * 256, (n + 1) * 256)
            acc = sums_in[:, cols] + chunk(spans[5:], cols)
            hidden[:, n * 128 : (n + 1) * 128] = (jax.nn.silu(acc[:, 0:128]) * acc[:, 128:256]).astype(BF)

    def down():
        acc = jnp.dot(first[...].reshape(512, 2048), wd[:, 11:13].reshape(2048, 128), preferred_element_type=F32)
        prod = jax.nn.silu(acc) * pltpu.roll(acc, 64, axis=1)
        real = lax.broadcasted_iota(jnp.int32, (512, 128), 1) < 64
        hidden[:, 640:768] = jnp.where(real, prod, 0.0).astype(BF)
        for d in (2, 1, 3, 0):
            xb = wrap(me.x + d, XN)
            for b, swap in ((xb * 2 + 1 - me.c, True), (xb * 2 + me.c, False)):
                shards = pl.ds(b * 8, 8)
                cols = [wd[shards, 2 * n : 2 * n + 2].reshape(256, 128) for n in range(5)]
                both = wd[shards, 10].reshape(128, 128)
                turned = pltpu.roll(both.astype(F32), 64, axis=1).astype(BF)
                cols.append(jnp.stack([both.reshape(8, 16, 128), turned.reshape(8, 16, 128)], axis=1).reshape(256, 128))
                part2[b] = nt_dot(hidden[...], jnp.concatenate(cols, axis=1)).astype(BF)
                if swap:
                    rs2.swap(d)
            if d == 3:
                rs2.far()
        rs2.near()
        rs2.hop()

    def norm_two():
        here = pl.ds(pl.multiple_of(me.t * 256, 256), 256)
        second = ALPHA * first[:, :, here].reshape(512, 256).astype(F32) + rs2.result()
        stat2[me.t] = jnp.concatenate([row_sums(second), row_sums(second * second)], axis=0)
        everyone(me, stat2, st2_s, one.at[16])
        from_everyone(me, stat2, st2_s)
        sums = jnp.sum(stat2[...], axis=0)
        mean = sums[0:1] / 2048.0
        rstd = lax.rsqrt(sums[1:2] / 2048.0 - mean * mean + EPS)
        mean, rstd = spread(mean), spread(rstd)
        for k in range(2):
            span = slice(k * 128, (k + 1) * 128)
            out[:, span] = ((second[:, span] - mean) * rstd * g2[:, span]).astype(BF)

    parts = {
        "uv": uv, "wo": wo_g, "gu": gu, "dn": dn, "ag1": ag1, "ag2": ag2, "rs1": rs1,
        "pack": pack, "branches": branches, "gate": gate, "norm_one": norm_one, "near": hidden_near,
        "far": hidden_far, "down": down, "norm_two": norm_two,
    }

    def act(name, method=None, *at):
        part = parts[name]
        if (name, method) == ("ag1", "start"):
            loads[3].wait()
        (part if method is None else getattr(part, method))(*at)

    for step in ORDER:
        act(*step)

    for each in (uv, wo_g, gu, dn, ag1, ag2, rs1, rs2):
        each.drain()
    drain_everyone(me, gains, one.at[14])
    drain_everyone(me, stat1, one.at[15])
    drain_everyone(me, stat2, one.at[16])


def on_device(tokens, u, v, sgg, sw, sb, ow, g1, gw, uw, dw, g2):
    vmem = pltpu.VMEM
    dma = pltpu.SemaphoreType.DMA
    scatter1 = [vmem((8, 64, 2048), BF), vmem((4, 64, 2048), BF), vmem((4, 64, 2048), BF), vmem((2, 32, 2048), BF), vmem((2, 64, 2048), BF)]
    scatter2 = [vmem((8, 512, 256), BF), vmem((4, 512, 256), BF), vmem((4, 512, 256), BF), vmem((2, 256, 256), BF), vmem((2, 512, 256), BF)]
    scratch = [
        vmem((2048, 256), BF), vmem((2048, 128), BF), vmem((2048, 1280), BF), vmem((64, 13, 16, 128), BF),
        vmem((8, 512, 256), BF), vmem((8, 64, 2048), BF), vmem((8, 1, 256), F32), vmem((8, 2, 512), F32), vmem((8, 2, 512), F32),
        *scatter1, *scatter2,
        vmem((512, 128), F32), vmem((512, 128), F32), vmem((512, 128), BF), vmem((512, 1280), F32), vmem((512, 768), BF),
        vmem((1, 128), F32), vmem((1, 128, 128), BF), vmem((1, 128), F32),
        vmem((32, 704), BF), vmem((32, 704), BF), vmem((32, 704), BF), vmem((1, 256), F32),
        *[dma((9,)) for _ in range(12)],
        dma((4,)), dma((18,)), dma((18,)),
        dma((6,)), dma((6,)), dma((10,)), dma((10,)), dma((8,)), dma((8,)), dma((8,)), dma((17,)), dma((12,)),
    ]
    args = (tokens, u, v, sgg.reshape(1, -1), sw, sb, ow.T, g1.reshape(1, -1), gw, uw, dw.T, g2.reshape(1, -1))
    args = [pltpu.with_memory_space_constraint(each, pltpu.HBM) for each in args]
    return pl.pallas_call(
        kernel,
        out_shape=jax.ShapeDtypeStruct((512, 256), BF),
        in_specs=[pl.BlockSpec(memory_space=pltpu.HBM)] * 12,
        out_specs=pl.BlockSpec(memory_space=pltpu.VMEM),
        scratch_shapes=scratch,
        compiler_params=pltpu.CompilerParams(collective_id=0, has_side_effects=True, vmem_limit_bytes=40 * 1024 * 1024),
    )(*args)


def solution(mesh):
    fs_tp, tp = P("fs", "tp"), P("tp")
    return jax.shard_map(
        on_device,
        mesh=mesh,
        in_specs=(
            fs_tp, fs_tp, fs_tp, tp, P("tp", None, None), P("tp", None), P("tp", "fs"), tp, fs_tp, fs_tp, P("tp", "fs"), tp,
        ),
        out_specs=fs_tp,
        check_vma=False,
    )
```

```python
import jax
import jax.numpy as jnp
from jax import lax
from jax.experimental import pallas as pl
from jax.experimental.pallas import tpu as pltpu
from jax.sharding import PartitionSpec as P

EPS = 1e-05
ALPHA = 2.0**0.25
MESH = pl.DeviceIdType.MESH
ZN, YN, XN = 16, 4, 4
BF, F32 = jnp.bfloat16, jnp.float32
UV_DIRECT, WO_DIRECT, UV_HOPS, WO_HOPS = 9, 9, 2, 2
ORDER = (
    ("ag1", "start"), ("uv", "z", 0), ("uv", "ys", 0), ("wo", "z", 0), ("wo", "ys", 0), ("pack",), ("dn", "y0"),
    ("gu", "z", 0), ("gu", "ys", 0), ("uv", "z", 1), ("uv", "ys", 1), ("wo", "z", 1), ("wo", "ys", 1), ("dn", "y1"),
    ("uv", "yf", 0), ("uv", "z", 2), ("wo", "z", 2), ("uv", "ys", 2), ("gu", "z", 1), ("gu", "ys", 1), ("uv", "z", 3),
    ("wo", "ys", 2), ("wo", "z", 3), ("wo", "ys", 3), ("uv", "yf", 1), ("dn", "y2"), ("uv", "z", 4), ("uv", "yf", 2),
    ("wo", "z", 4), ("uv", "ys", 3), ("uv", "ys", 4), ("ag1", "forward"), ("dn", "z", 0, 0), ("uv", "z", 5),
    ("gu", "z", 2), ("wo", "yf", 0), ("uv", "ys", 5), ("wo", "ys", 4), ("gu", "ys", 2), ("wo", "yf", 1),
    ("uv", "z", 6), ("ag1", "middle"), ("uv", "ys", 6), ("wo", "yf", 2), ("uv", "yf", 3), ("wo", "z", 5),
    ("wo", "z", 6), ("dn", "z", 0, 1), ("uv", "z", 7), ("ag1", "end"), ("uv", "ys", 7), ("gu", "z", 3),
    ("uv", "z", 8), ("uv", "ys", 8), ("wo", "ys", 5), ("wo", "z", 7), ("wo", "ys", 6), ("dn", "z", 1, 0),
    ("ag1", "finish"), ("uv", "yf", 4), ("uv", "yf", 5), ("dn", "z", 1, 1), ("wo", "z", 8), ("wo", "ys", 7),
    ("wo", "ys", 8), ("uv", "yf", 6), ("uv", "yf", 7), ("uv", "yf", 8), ("gu", "ys", 3), ("gu", "yf", 0),
    ("wo", "yf", 3), ("wo", "yf", 4), ("wo", "yf", 5), ("gu", "z", 4), ("dn", "z", 2, 0), ("wo", "yf", 6),
    ("wo", "yf", 7), ("wo", "yf", 8), ("branches",), ("gu", "ys", 4), ("dn", "z", 2, 1), ("gu", "z", 5),
    ("dn", "z", 3, 0), ("gu", "yf", 1), ("gu", "yf", 2), ("gu", "ys", 5), ("gate",), ("dn", "z", 3, 1),
    ("rs1", "far"), ("rs1", "near"), ("dn", "z", 4, 0), ("gu", "yf", 3), ("gu", "z", 6), ("gu", "yf", 4),
    ("gu", "ys", 6), ("rs1", "hop"), ("dn", "z", 4, 1), ("dn", "z", 5, 0), ("gu", "z", 7), ("gu", "ys", 7),
    ("norm_one",), ("gu", "yf", 5), ("dn", "z", 5, 1), ("dn", "z", 6, 0), ("gu", "z", 8), ("gu", "ys", 8),
    ("ag2", "forward"), ("dn", "z", 6, 1), ("gu", "yf", 6), ("gu", "yf", 7), ("dn", "z", 7, 0), ("gu", "yf", 8),
    ("ag2", "middle"), ("ag2", "end"), ("dn", "z", 7, 1), ("ag2", "finish"), ("near",), ("far",), ("dn", "z", 8, 0),
    ("dn", "z", 8, 1), ("down",), ("norm_two",),
)


def wrap(value, size):
    return lax.rem(value + size, size)


def nt_dot(left, right, **kw):
    return lax.dot_general(left, right, (((1,), (1,)), ((), ())), preferred_element_type=F32, **kw)


class Place:
    def __init__(self):
        f, t = lax.axis_index("fs"), lax.axis_index("tp")
        self.f, self.t = f, t
        self.z, self.y = lax.div(f, YN), lax.rem(f, YN)
        self.x, self.c = lax.div(t, 2), lax.rem(t, 2)
        self.zp = (wrap(self.z + 1, ZN) * YN + self.y, t)
        self.zm = (wrap(self.z - 1, ZN) * YN + self.y, t)
        self.yp = (self.z * YN + wrap(self.y + 1, YN), t)
        self.ym = (self.z * YN + wrap(self.y - 1, YN), t)
        self.y2 = (self.z * YN + wrap(self.y + 2, YN), t)
        self.xp = (f, wrap(self.x + 1, XN) * 2 + self.c)
        self.xm = (f, wrap(self.x - 1, XN) * 2 + self.c)
        self.mate = (f, self.x * 2 + 1 - self.c)

    def along_z(self, n):
        return (wrap(self.z + n, ZN) * YN + self.y, self.t)


def copy_to(src, dst, send, recv, dev):
    pltpu.make_async_remote_copy(src_ref=src, dst_ref=dst, send_sem=send, recv_sem=recv, device_id=dev, device_id_type=MESH).start()


def await_recv(dst, recv, dev):
    pltpu.make_async_remote_copy(src_ref=dst, dst_ref=dst, send_sem=recv, recv_sem=recv, device_id=dev, device_id_type=MESH).wait_recv()


def await_send(src, send, dev):
    pltpu.make_async_remote_copy(src_ref=src, dst_ref=src, send_sem=send, recv_sem=send, device_id=dev, device_id_type=MESH).wait_send()


class ZThenY:
    def __init__(self, w, f_sem, b_sem, yf_sem, yb_sem, last, sent, me, hops=1, split=9, direct=9):
        self.w, self.f_sem, self.b_sem, self.yf_sem, self.yb_sem = w, f_sem, b_sem, yf_sem, yb_sem
        self.last, self.sent, self.me, self.hops, self.split, self.direct = last, sent, me, hops, split, direct

    def block(self, zb, yb):
        row = (wrap(zb, ZN) * YN + wrap(yb, YN)) * 32
        return self.w.at[pl.ds(pl.multiple_of(row, 32), 32), :]

    def side(self, block, s, h):
        return block.at[pl.ds(h * 16, 16), :] if s == 8 else block

    def final(self, s):
        return self.last.at[0 if s < self.split else 1]

    def z(self, s):
        me = self.me
        fwd, bwd = self.block(me.z - s, me.y), self.block(me.z + s, me.y)
        steps = range(1, self.hops + 1) if s == 0 else (self.hops,)
        if s > 0:
            await_recv(self.side(fwd, s, 0), self.f_sem.at[s], me.zm)
        for n in steps:
            if s + n <= 8:
                part = self.side(fwd, s + n, 0)
                copy_to(part, part, self.sent, self.f_sem.at[s + n], me.along_z(n))
        if s > 0:
            await_recv(self.side(bwd, s, 1), self.b_sem.at[s], me.zp)
        for n in steps:
            if s + n <= 8:
                part = self.side(bwd, s + n, 1)
                copy_to(part, part, self.sent, self.b_sem.at[s + n], me.along_z(-n))

    def up(self, s, block):
        me = self.me
        copy_to(block, block, self.sent, self.yf_sem.at[s], me.yp)
        copy_to(block, block, self.sent, self.final(s), me.ym)

    def down(self, s, block):
        me = self.me
        copy_to(block, block, self.sent, self.yb_sem.at[s], me.ym)
        copy_to(block, block, self.sent, self.final(s), me.yp)

    def ys(self, s):
        me = self.me
        if s >= self.direct:
            for zb in (me.z - s, me.z + s)[: 1 if s in (0, 8) else 2]:
                block = self.block(zb, me.y)
                for dev in (me.yp, me.ym, me.y2):
                    copy_to(block, block, self.sent, self.final(s), dev)
            return
        if s < 8:
            self.up(s, self.block(me.z - s, me.y))
        if s > 0:
            self.down(s, self.block(me.z + s, me.y))

    def yf(self, s):
        me = self.me
        if s < 8:
            block = self.block(me.z - s, me.y - 1)
            await_recv(block, self.yf_sem.at[s], me.ym)
            copy_to(block, block, self.sent, self.final(s), me.yp)
        if s > 0:
            block = self.block(me.z + s, me.y + 1)
            await_recv(block, self.yb_sem.at[s], me.yp)
            copy_to(block, block, self.sent, self.final(s), me.ym)

    def finish(self, part=0):
        total = 0
        for s in range(9):
            if (s >= self.split) == (part == 1):
                total += (1 if s in (0, 8) else 2) * (3 if s >= self.direct else 2)
        await_recv(self.w.at[pl.ds(0, total * 32), :], self.last.at[part], self.me.yp)

    def drain(self):
        await_send(self.w.at[pl.ds(0, 2016), :], self.sent, self.me.yp)


class YThenZ:
    def __init__(self, w, y_sem, f_sem, b_sem, sent, me):
        self.w, self.y_sem, self.f_sem, self.b_sem, self.sent, self.me = w, y_sem, f_sem, b_sem, sent, me

    def shard(self, yb, start=0, size=13):
        return self.w.at[self.me.z * YN + wrap(yb, YN), pl.ds(start, size)]

    def block(self, zb, h):
        return self.w.at[pl.ds(wrap(zb, ZN) * 4 + h * 2, 2)]

    def y0(self):
        me = self.me
        own = self.shard(me.y)
        copy_to(own, own, self.sent, self.y_sem.at[0], me.yp)
        copy_to(own, own, self.sent, self.y_sem.at[1], me.ym)

    def y1(self):
        me = self.me
        await_recv(self.shard(me.y - 1), self.y_sem.at[0], me.ym)
        half = self.shard(me.y - 1, 0, 7)
        copy_to(half, half, self.sent, self.y_sem.at[2], me.yp)
        await_recv(self.shard(me.y + 1), self.y_sem.at[1], me.yp)
        half = self.shard(me.y + 1, 7, 6)
        copy_to(half, half, self.sent, self.y_sem.at[3], me.ym)

    def y2(self):
        me = self.me
        await_recv(self.shard(me.y - 2, 0, 7), self.y_sem.at[2], me.ym)
        await_recv(self.shard(me.y + 2, 7, 6), self.y_sem.at[3], me.yp)

    def z(self, s, h):
        me = self.me
        fwd, bwd = self.block(me.z - s, h), self.block(me.z + s, h)
        if 0 < s < 8 or (s == 8 and h == 0):
            await_recv(fwd, self.f_sem.at[h * 9 + s], me.zm)
        if s < 7 or (s == 7 and h == 0):
            copy_to(fwd, fwd, self.sent, self.f_sem.at[h * 9 + s + 1], me.zp)
        if 0 < s < 8 or (s == 8 and h == 1):
            await_recv(bwd, self.b_sem.at[h * 9 + s], me.zp)
        if s < 7 or (s == 7 and h == 1):
            copy_to(bwd, bwd, self.sent, self.b_sem.at[h * 9 + s + 1], me.zm)

    def drain(self):
        await_send(self.w.at[pl.ds(0, 63)], self.sent, self.me.yp)


class Gather:
    def __init__(self, buf, sem, relayed, sent, me):
        self.buf, self.sem, self.relayed, self.sent, self.me = buf, sem, relayed, sent, me
        self.half = buf.shape[1] // 2

    def part(self, xb, h):
        b = wrap(xb, XN) * 2 + self.me.c
        return self.buf.at[b, pl.ds(h * self.half, self.half), :]

    def send(self, xb, h, sem, dev):
        part = self.part(xb, h)
        copy_to(part, part, self.sent, sem, dev)

    def take(self, xb, h, sem, dev):
        await_recv(self.part(xb, h), sem, dev)

    def start(self):
        me = self.me
        self.send(me.x, 0, self.sem.at[0], me.xp)
        self.send(me.x, 1, self.sem.at[3], me.xm)
        self.send(me.x, 1, self.sem.at[1], me.xp)
        self.send(me.x, 0, self.sem.at[2], me.xm)
        own = self.buf.at[me.t]
        copy_to(own, own, self.sent, self.relayed, me.mate)

    def forward(self):
        me = self.me
        self.take(me.x - 1, 0, self.sem.at[0], me.xm)
        self.send(me.x - 1, 0, self.sem.at[4], me.xp)
        self.send(me.x - 1, 0, self.relayed, me.mate)
        self.take(me.x + 1, 1, self.sem.at[3], me.xp)
        self.send(me.x + 1, 1, self.sem.at[5], me.xm)
        self.send(me.x + 1, 1, self.relayed, me.mate)

    def middle(self):
        me = self.me
        self.take(me.x - 1, 1, self.sem.at[1], me.xm)
        self.send(me.x - 1, 1, self.relayed, me.mate)
        self.take(me.x + 1, 0, self.sem.at[2], me.xp)
        self.send(me.x + 1, 0, self.relayed, me.mate)

    def end(self):
        me = self.me
        self.take(me.x - 2, 0, self.sem.at[4], me.xm)
        self.send(me.x - 2, 0, self.relayed, me.mate)
        self.take(me.x + 2, 1, self.sem.at[5], me.xp)
        self.send(me.x + 2, 1, self.relayed, me.mate)

    def finish(self):
        await_recv(self.buf.at[pl.ds(0, 4)], self.relayed, self.me.mate)

    def drain(self):
        await_send(self.buf.at[pl.ds(0, 7)], self.sent, self.me.mate)


class Scatter:
    def __init__(self, part, other, total, via, got, sem, sent, me):
        self.part, self.other, self.total, self.via, self.got = part, other, total, via, got
        self.sem, self.sent, self.me = sem, sent, me
        self.half = part.shape[1] // 2

    def swap(self, d):
        me = self.me
        xb = wrap(me.x + d, XN)
        copy_to(self.part.at[xb * 2 + 1 - me.c], self.other.at[d], self.sent, self.sem.at[d], me.mate)

    def add(self, d):
        me = self.me
        xb = wrap(me.x + d, XN)
        await_recv(self.other.at[d], self.sem.at[d], me.mate)
        return self.part[xb * 2 + me.c].astype(F32) + self.other[d].astype(F32)

    def rows(self, h):
        return pl.ds(h * self.half, self.half)

    def far(self):
        me = self.me
        self.total[2] = self.add(2).astype(BF)
        copy_to(self.total.at[2, self.rows(0), :], self.via.at[0], self.sent, self.sem.at[4], me.xp)
        copy_to(self.total.at[2, self.rows(1), :], self.via.at[1], self.sent, self.sem.at[5], me.xm)

    def near(self):
        me = self.me
        self.total[1] = self.add(1).astype(BF)
        copy_to(self.total.at[1, self.rows(1), :], self.got.at[0, self.rows(1), :], self.sent, self.sem.at[6], me.xp)
        self.total[3] = self.add(3).astype(BF)
        copy_to(self.total.at[3, self.rows(0), :], self.got.at[1, self.rows(0), :], self.sent, self.sem.at[7], me.xm)

    def hop(self):
        me = self.me
        await_recv(self.via.at[0], self.sem.at[4], me.xm)
        self.total[1, self.rows(0), :] = (self.total[1, self.rows(0), :].astype(F32) + self.via[0].astype(F32)).astype(BF)
        copy_to(self.total.at[1, self.rows(0), :], self.got.at[0, self.rows(0), :], self.sent, self.sem.at[8], me.xp)
        await_recv(self.via.at[1], self.sem.at[5], me.xp)
        self.total[3, self.rows(1), :] = (self.total[3, self.rows(1), :].astype(F32) + self.via[1].astype(F32)).astype(BF)
        copy_to(self.total.at[3, self.rows(1), :], self.got.at[1, self.rows(1), :], self.sent, self.sem.at[9], me.xm)

    def result(self):
        me = self.me
        own = self.add(0)
        await_recv(self.got.at[0, self.rows(1), :], self.sem.at[6], me.xm)
        await_recv(self.got.at[1, self.rows(0), :], self.sem.at[7], me.xp)
        top = own[: self.half] + self.got[1, self.rows(0), :].astype(F32)
        bottom = own[self.half :] + self.got[0, self.rows(1), :].astype(F32)
        await_recv(self.got.at[0, self.rows(0), :], self.sem.at[8], me.xm)
        top = top + self.got[0, self.rows(0), :].astype(F32)
        await_recv(self.got.at[1, self.rows(1), :], self.sem.at[9], me.xp)
        bottom = bottom + self.got[1, self.rows(1), :].astype(F32)
        return jnp.concatenate([top, bottom], axis=0).astype(BF).astype(F32)

    def drain(self):
        await_send(self.part.at[pl.ds(0, 7)], self.sent, self.me.mate)


def everyone(me, buf, recv, sent):
    own = buf.at[me.t]
    for d in (4, 3, 5, 2, 6, 1, 7):
        copy_to(own, own, sent, recv.at[d], (me.f, wrap(me.t + d, 8)))


def from_everyone(me, buf, recv):
    for d in range(1, 8):
        t = wrap(me.t - d, 8)
        await_recv(buf.at[t], recv.at[d], (me.f, t))


def drain_everyone(me, buf, sent):
    await_send(buf.at[pl.ds(0, 7)], sent, (me.f, wrap(me.t + 1, 8)))


def row_sums(vals):
    folded = vals[:, 0:128]
    for k in range(1, vals.shape[1] // 128):
        folded = folded + vals[:, k * 128 : (k + 1) * 128]
    return jnp.sum(folded.T, axis=0, keepdims=True)


def spread(line, rows=128):
    return jnp.broadcast_to(line, (rows, line.shape[1])).T


def kernel(
    tok, u, v, sgg_in, sw_in, sb_in, ow, g1, gw_in, uw_in, dw_in, g2_in, out,
    wuv, wo, wgu, wd, tall, first, gains, stat1, stat2,
    part1, other1, total1, via1, got1, part2, other2, total2, via2, got2,
    gated, valued, mixed_in, sums_in, hidden, sgg, sw, sb, gw, uw, dw, g2,
    uv_f, uv_b, uv_yf, uv_yb, wo_f, wo_b, wo_yf, wo_yb, gu_f, gu_b, gu_yf, gu_yb, wd_y, wd_f, wd_b,
    ag1_s, ag2_s, rs1_s, rs2_s, gain_s, st1_s, st2_s, one, in_s,
):
    me = Place()
    barrier = pltpu.get_barrier_semaphore()
    for dev in (me.zp, me.zm, me.along_z(2), me.along_z(-2), me.yp, me.ym, me.y2):
        pl.semaphore_signal(barrier, inc=1, device_id=dev, device_id_type=MESH)
    for d in range(1, 8):
        pl.semaphore_signal(barrier, inc=1, device_id=(me.f, wrap(me.t + d, 8)), device_id_type=MESH)

    rows = pl.ds(pl.multiple_of(me.f * 32, 32), 32)
    loads = [
        pltpu.make_async_copy(src, dst, in_s.at[k])
        for k, (src, dst) in enumerate(
            (
                (u, wuv.at[rows, pl.ds(0, 128)]), (v, wuv.at[rows, pl.ds(128, 128)]), (ow, wo.at[rows, :]),
                (tok, tall.at[me.t]), (g1, gains.at[me.t]), (gw_in, gw), (uw_in, uw), (dw_in, dw),
                (sgg_in, sgg), (sw_in, sw), (sb_in, sb), (g2_in, g2),
            )
        )
    ]
    for load in loads:
        load.start()
    for load in loads[:3]:
        load.wait()
    pl.semaphore_wait(barrier, 14)

    uv = ZThenY(wuv, uv_f, uv_b, uv_yf, uv_yb, one.at[pl.ds(0, 1)], one.at[1], me, hops=UV_HOPS, direct=UV_DIRECT)
    wo_g = ZThenY(wo, wo_f, wo_b, wo_yf, wo_yb, one.at[pl.ds(2, 1)], one.at[3], me, hops=WO_HOPS, direct=WO_DIRECT)
    gu = ZThenY(wgu, gu_f, gu_b, gu_yf, gu_yb, one.at[pl.ds(4, 2)], one.at[6], me, split=7)
    dn = YThenZ(wd, wd_y, wd_f, wd_b, one.at[7], me)
    ag1 = Gather(tall, ag1_s, one.at[8], one.at[9], me)
    ag2 = Gather(first, ag2_s, one.at[10], one.at[11], me)
    rs1 = Scatter(part1, other1, total1, via1, got1, rs1_s, one.at[12], me)
    rs2 = Scatter(part2, other2, total2, via2, got2, rs2_s, one.at[13], me)
    pairs = [wrap(lax.div(me.z, 2) + lax.rem(me.z, 2) + j, 8) * 256 for j in (-3, -2, -1, 0, 1, 2, 3, 4)]
    spans = [pl.ds(pl.multiple_of(p, 256), 256) for p in pairs]

    def pack():
        for load in loads[4:]:
            load.wait()
        lane = lax.broadcasted_iota(jnp.int32, (64, 128), 1)
        line = lax.broadcasted_iota(jnp.int32, (64, 128), 0)
        low, high = (lane == line).astype(BF), (lane == line + 64).astype(BF)
        for n in range(5):
            wgu[rows, n * 256 : n * 256 + 128] = gw[:, n * 128 : (n + 1) * 128]
            wgu[rows, n * 256 + 128 : n * 256 + 256] = uw[:, n * 128 : (n + 1) * 128]
        tail = jnp.dot(gw[:, 640:704], low, preferred_element_type=F32) + jnp.dot(uw[:, 640:704], high, preferred_element_type=F32)
        wd[me.f, 11:13] = tail.astype(BF).reshape(2, 16, 128)
        for n in range(5):
            wd[me.f, 2 * n : 2 * n + 2] = dw[:, n * 128 : (n + 1) * 128].reshape(2, 16, 128)
        both = jnp.dot(dw[0:16, 640:704], low, preferred_element_type=F32) + jnp.dot(dw[16:32, 640:704], high, preferred_element_type=F32)
        wd[me.f, 10] = both.astype(BF)

    def branches():
        uv.finish()
        left = jnp.concatenate([tall[k] for k in range(8)], axis=1)
        val = jax.nn.gelu(jnp.dot(left, wuv[:, 128:256], preferred_element_type=F32))
        valued[...] = val
        stat1[me.t] = jnp.concatenate([row_sums(val), row_sums(val * val)], axis=0)
        everyone(me, stat1, st1_s, one.at[15])
        everyone(me, gains, gain_s, one.at[14])
        gated[...] = jax.nn.gelu(jnp.dot(left, wuv[:, 0:128], preferred_element_type=F32))

    def gate():
        from_everyone(me, stat1, st1_s)
        sums = jnp.sum(stat1[...], axis=0)
        mean = sums[0:1] / 1024.0
        rstd = lax.rsqrt(sums[1:2] / 1024.0 - mean * mean + EPS)
        normed = ((valued[...] - spread(mean)) * spread(rstd) * sgg[...]).astype(BF)
        keep = lax.broadcasted_iota(jnp.int32, (128, 128), 0) >= lax.broadcasted_iota(jnp.int32, (128, 128), 1)
        mask = jnp.where(keep, sw[0].astype(F32), 0.0).astype(BF)
        bias = spread(sb[...])
        wide = jnp.concatenate([normed[k * 128 : (k + 1) * 128] for k in range(4)], axis=1)
        mixed = jnp.dot(mask, wide, preferred_element_type=F32)
        for k in range(4):
            span = slice(k * 128, (k + 1) * 128)
            mixed_in[span, :] = (gated[span, :] * (mixed[:, span] + bias)).astype(BF)
        wo_g.finish()
        for d in (2, 1, 3, 0):
            xb = wrap(me.x + d, XN)
            left = mixed_in[pl.ds(pl.multiple_of(xb * 128, 128), 128), :]
            part1[pl.ds(xb * 2, 2)] = nt_dot(left, wo[...]).astype(BF).reshape(2, 64, 2048)
            rs1.swap(d)

    def norm_one():
        mine = pl.ds(pl.multiple_of(me.t * 64, 64), 64)
        held = jnp.concatenate([tall[k, mine, :] for k in range(8)], axis=1).astype(F32)
        resid = ALPHA * held + rs1.result()
        from_everyone(me, gains, gain_s)
        gain = jnp.concatenate([gains[k] for k in range(8)], axis=1)
        mean = jnp.sum(resid, axis=1, keepdims=True) / 2048.0
        square = jnp.sum(resid * resid, axis=1, keepdims=True) / 2048.0
        first[me.t] = ((resid - mean) * lax.rsqrt(square - mean * mean + EPS) * gain).astype(BF)
        ag2.start()

    def chunk(spans, cols):
        left = jnp.concatenate([first[:, :, span].reshape(512, 256) for span in spans], axis=1)
        right = jnp.concatenate([wgu[span, cols] for span in spans], axis=0)
        return jnp.dot(left, right, preferred_element_type=F32)

    def hidden_near():
        gu.finish()
        for n in range(5):
            sums_in[:, n * 256 : (n + 1) * 256] = chunk(spans[:6], slice(n * 256, (n + 1) * 256))

    def hidden_far():
        gu.finish(1)
        for n in range(5):
            cols = slice(n * 256, (n + 1) * 256)
            acc = sums_in[:, cols] + chunk(spans[6:], cols)
            hidden[:, n * 128 : (n + 1) * 128] = (jax.nn.silu(acc[:, 0:128]) * acc[:, 128:256]).astype(BF)

    def down():
        acc = jnp.dot(first[...].reshape(512, 2048), wd[:, 11:13].reshape(2048, 128), preferred_element_type=F32)
        prod = jax.nn.silu(acc) * pltpu.roll(acc, 64, axis=1)
        real = lax.broadcasted_iota(jnp.int32, (512, 128), 1) < 64
        hidden[:, 640:768] = jnp.where(real, prod, 0.0).astype(BF)
        for d in (2, 1, 3, 0):
            xb = wrap(me.x + d, XN)
            for b, swap in ((xb * 2 + 1 - me.c, True), (xb * 2 + me.c, False)):
                shards = pl.ds(b * 8, 8)
                cols = [wd[shards, 2 * n : 2 * n + 2].reshape(256, 128) for n in range(5)]
                both = wd[shards, 10].reshape(128, 128)
                turned = pltpu.roll(both.astype(F32), 64, axis=1).astype(BF)
                cols.append(jnp.stack([both.reshape(8, 16, 128), turned.reshape(8, 16, 128)], axis=1).reshape(256, 128))
                part2[b] = nt_dot(hidden[...], jnp.concatenate(cols, axis=1)).astype(BF)
                if swap:
                    rs2.swap(d)
            if d == 3:
                rs2.far()
        rs2.near()
        rs2.hop()

    def norm_two():
        here = pl.ds(pl.multiple_of(me.t * 256, 256), 256)
        second = ALPHA * first[:, :, here].reshape(512, 256).astype(F32) + rs2.result()
        stat2[me.t] = jnp.concatenate([row_sums(second), row_sums(second * second)], axis=0)
        everyone(me, stat2, st2_s, one.at[16])
        from_everyone(me, stat2, st2_s)
        sums = jnp.sum(stat2[...], axis=0)
        mean = sums[0:1] / 2048.0
        rstd = lax.rsqrt(sums[1:2] / 2048.0 - mean * mean + EPS)
        mean, rstd = spread(mean), spread(rstd)
        for k in range(2):
            span = slice(k * 128, (k + 1) * 128)
            out[:, span] = ((second[:, span] - mean) * rstd * g2[:, span]).astype(BF)

    parts = {
        "uv": uv, "wo": wo_g, "gu": gu, "dn": dn, "ag1": ag1, "ag2": ag2, "rs1": rs1,
        "pack": pack, "branches": branches, "gate": gate, "norm_one": norm_one, "near": hidden_near,
        "far": hidden_far, "down": down, "norm_two": norm_two,
    }

    def act(name, method=None, *at):
        part = parts[name]
        if (name, method) == ("ag1", "start"):
            loads[3].wait()
        (part if method is None else getattr(part, method))(*at)

    for step in ORDER:
        act(*step)

    for each in (uv, wo_g, gu, dn, ag1, ag2, rs1, rs2):
        each.drain()
    drain_everyone(me, gains, one.at[14])
    drain_everyone(me, stat1, one.at[15])
    drain_everyone(me, stat2, one.at[16])


def on_device(tokens, u, v, sgg, sw, sb, ow, g1, gw, uw, dw, g2):
    vmem = pltpu.VMEM
    dma = pltpu.SemaphoreType.DMA
    scatter1 = [vmem((8, 64, 2048), BF), vmem((4, 64, 2048), BF), vmem((4, 64, 2048), BF), vmem((2, 32, 2048), BF), vmem((2, 64, 2048), BF)]
    scatter2 = [vmem((8, 512, 256), BF), vmem((4, 512, 256), BF), vmem((4, 512, 256), BF), vmem((2, 256, 256), BF), vmem((2, 512, 256), BF)]
    scratch = [
        vmem((2048, 256), BF), vmem((2048, 128), BF), vmem((2048, 1280), BF), vmem((64, 13, 16, 128), BF),
        vmem((8, 512, 256), BF), vmem((8, 64, 2048), BF), vmem((8, 1, 256), F32), vmem((8, 2, 512), F32), vmem((8, 2, 512), F32),
        *scatter1, *scatter2,
        vmem((512, 128), F32), vmem((512, 128), F32), vmem((512, 128), BF), vmem((512, 1280), F32), vmem((512, 768), BF),
        vmem((1, 128), F32), vmem((1, 128, 128), BF), vmem((1, 128), F32),
        vmem((32, 704), BF), vmem((32, 704), BF), vmem((32, 704), BF), vmem((1, 256), F32),
        *[dma((9,)) for _ in range(12)],
        dma((4,)), dma((18,)), dma((18,)),
        dma((6,)), dma((6,)), dma((10,)), dma((10,)), dma((8,)), dma((8,)), dma((8,)), dma((17,)), dma((12,)),
    ]
    args = (tokens, u, v, sgg.reshape(1, -1), sw, sb, ow.T, g1.reshape(1, -1), gw, uw, dw.T, g2.reshape(1, -1))
    args = [pltpu.with_memory_space_constraint(each, pltpu.HBM) for each in args]
    return pl.pallas_call(
        kernel,
        out_shape=jax.ShapeDtypeStruct((512, 256), BF),
        in_specs=[pl.BlockSpec(memory_space=pltpu.HBM)] * 12,
        out_specs=pl.BlockSpec(memory_space=pltpu.VMEM),
        scratch_shapes=scratch,
        compiler_params=pltpu.CompilerParams(collective_id=0, has_side_effects=True, vmem_limit_bytes=40 * 1024 * 1024),
    )(*args)


def solution(mesh):
    fs_tp, tp = P("fs", "tp"), P("tp")
    return jax.shard_map(
        on_device,
        mesh=mesh,
        in_specs=(
            fs_tp, fs_tp, fs_tp, tp, P("tp", None, None), P("tp", None), P("tp", "fs"), tp, fs_tp, fs_tp, P("tp", "fs"), tp,
        ),
        out_specs=fs_tp,
        check_vma=False,
    )
```
